512 devices in a mesh: sp: 16 (over y, x), tp: 32 (over z, core).
Axes of the slice: x: 4, y: 4, z: 16, core: 2. Of those that a mesh axis runs over, the one named last changes fastest.
Arguments:
- target: bfloat16 [2048, 2048], P('sp'), may hold values from -6 to 6
- source: bfloat16 [6144, 2048], P('sp'), may hold values from -6 to 6
- cotangent: bfloat16 [2048, 2048], P('sp'), may hold values from -192 to 192
- target_gain: float32 [2048], replicated, may hold values from 0.1 to 1.9
- source_gain: float32 [2048], replicated, may hold values from 0.1 to 1.9
- w_query: bfloat16 [2048, 4096], P(None, 'tp'), may hold values from -0.125 to 0.125
- w_key: bfloat16 [2048, 128], replicated, may hold values from -0.125 to 0.125
- w_value: bfloat16 [2048, 128], replicated, may hold values from -0.125 to 0.125
- w_out: bfloat16 [4096, 2048], P('tp'), may hold values from -0.09375 to 0.09375
Outputs:
- grad_target: bfloat16 [2048, 2048], P(('sp', 'tp'))
- grad_source: bfloat16 [6144, 2048], P(('sp', 'tp'))
- grad_out_w: bfloat16 [4096, 2048], P('tp', 'sp')
The draws below stay inside these ranges and needn't reach their ends.
All inputs are finite; a program needn't handle non-finite values.
Results may differ from the reference program's by a relative error of at most 0.025.
Values may be sent and summed in bfloat16 or wider, within the bound.
A program may use at most 64 MiB of HBM per device.

```python
import jax
import jax.numpy as jnp
from jax import lax

D = 2048
HEADS = 32
HEAD = 128
TARGET = 2048
SOURCE = 6144


def steps_of(own_key, dims, shards, low, largest):
    level = 1.0
    for dim, shards_of in shards:
        draws = jax.random.uniform(jax.random.fold_in(jax.random.fold_in(own_key, 6), dim), (shards_of,), jnp.float32, low / len(shards), largest / len(shards))
        level = level * jnp.repeat(jnp.exp(draws), dims[dim] // shards_of).reshape((-1,) + (1,) * (len(dims) - 1 - dim))
    return level


def bell_draw(own_key, extent, spread, bound, split=(), kind=jnp.bfloat16):
    result = spread * jax.random.normal(own_key, extent, jnp.float32)
    if split:
        result = result * steps_of(own_key, extent, split, -0.22, 0.18)
    return jnp.clip(result, -bound, bound).astype(kind)


def setup_inputs(seed: int = 0) -> dict:
    key_of = jax.random.split(jax.random.key(seed), 10)
    return {
        "target": bell_draw(key_of[0], (TARGET, D), 1.0, 6.0, ((0, 16),)),
        "source": bell_draw(key_of[1], (SOURCE, D), 1.0, 6.0, ((0, 16),)),
        "cotangent": bell_draw(key_of[2], (TARGET, D), 32.0, 192.0, ((0, 16),)),
        "target_gain": jnp.clip(1.0 + 0.18 * jax.random.normal(key_of[3], (D,), jnp.float32), 0.1, 1.9),
        "source_gain": jnp.clip(1.0 + 0.18 * jax.random.normal(key_of[4], (D,), jnp.float32), 0.1, 1.9),
        "w_query": bell_draw(key_of[5], (D, HEADS * HEAD), D ** -0.5, 0.125, ((1, 32),)),
        "w_key": bell_draw(key_of[6], (D, HEAD), D ** -0.5, 0.125),
        "w_value": bell_draw(key_of[7], (D, HEAD), D ** -0.5, 0.125),
        "w_out": bell_draw(key_of[8], (HEADS * HEAD, D), (HEADS * HEAD) ** -0.5, 0.09375, ((0, 32),)),
    }


NORM_EPS = 1e-06

def normed(row_block, gain_vec):
    rows_wide = row_block.astype(jnp.float32)
    inv_rms = lax.rsqrt(lax.optimization_barrier(jnp.mean(rows_wide * rows_wide, axis=1, keepdims=True)) + NORM_EPS)
    return (rows_wide * inv_rms * gain_vec).astype(jnp.bfloat16)

def norm_back(row_block, gain_vec, upstream):
    rows_wide = row_block.astype(jnp.float32)
    inv_rms = lax.rsqrt(lax.optimization_barrier(jnp.mean(rows_wide * rows_wide, axis=1, keepdims=True)) + NORM_EPS)
    unit_rows = rows_wide * inv_rms
    pulled = upstream * gain_vec
    return inv_rms * (pulled - unit_rows * lax.optimization_barrier(jnp.mean(pulled * unit_rows, axis=1, keepdims=True)))

def reference(target, source, cotangent, target_gain, source_gain, w_query, w_key, w_value, w_out):
    inv_root = HEAD ** (-0.5)
    normed_target = normed(target, target_gain)
    query_rows = jnp.dot(normed_target, w_query, preferred_element_type=jnp.float32).astype(jnp.bfloat16)
    normed_source = normed(source, source_gain)
    key_rows = jnp.dot(normed_source, w_key, preferred_element_type=jnp.float32).astype(jnp.bfloat16)
    value_rows = jnp.dot(normed_source, w_value, preferred_element_type=jnp.float32).astype(jnp.bfloat16)
    grad_attn = jnp.dot(cotangent, w_out.T, preferred_element_type=jnp.float32).astype(jnp.bfloat16)
    query_heads = query_rows.reshape(TARGET, HEADS, HEAD).transpose(1, 0, 2)
    grad_heads = grad_attn.reshape(TARGET, HEADS, HEAD).transpose(1, 0, 2)

    def one_head(carried, head_pair):
        key_sum, value_sum = carried
        query_one, grad_one = head_pair
        scores = jnp.dot(query_one, key_rows.T, preferred_element_type=jnp.float32) * inv_root
        exponent = jnp.exp(scores)
        row_total = lax.optimization_barrier(jnp.sum(exponent, axis=1))
        weights = exponent.astype(jnp.bfloat16)
        attended = (jnp.dot(weights, value_rows, preferred_element_type=jnp.float32) / row_total[:, None]).astype(jnp.bfloat16)
        prob_grad = jnp.dot(grad_one, value_rows.T, preferred_element_type=jnp.float32)
        delta_row = lax.optimization_barrier(jnp.sum(attended.astype(jnp.float32) * grad_one.astype(jnp.float32), axis=1))
        tilted = (exponent * prob_grad).astype(jnp.bfloat16)
        tilted_sum = jnp.dot(tilted, key_rows, preferred_element_type=jnp.float32)
        weight_sum = jnp.dot(weights, key_rows, preferred_element_type=jnp.float32)
        grad_query = ((tilted_sum - delta_row[:, None] * weight_sum) / row_total[:, None] * inv_root).astype(jnp.bfloat16)
        prob_rows = exponent / row_total[:, None]
        score_grad = (prob_rows * (prob_grad - delta_row[:, None])).astype(jnp.bfloat16)
        key_grad = jnp.dot(score_grad.T, query_one, preferred_element_type=jnp.float32) * inv_root
        value_grad = jnp.dot(prob_rows.astype(jnp.bfloat16).T, grad_one, preferred_element_type=jnp.float32)
        return ((key_sum + key_grad, value_sum + value_grad), (attended, grad_query))
    empty_keys = jnp.zeros((SOURCE, HEAD), jnp.float32)
    sums, stacked = lax.scan(one_head, (empty_keys, empty_keys), (query_heads, grad_heads))
    key_grad, value_grad = sums
    attended_heads, query_grad_heads = stacked
    attended_rows = attended_heads.transpose(1, 0, 2).reshape(TARGET, HEADS * HEAD)
    query_grad_rows = query_grad_heads.transpose(1, 0, 2).reshape(TARGET, HEADS * HEAD)
    pulled_source = jnp.dot(key_grad.astype(jnp.bfloat16), w_key.T, preferred_element_type=jnp.float32)
    pulled_source = pulled_source + jnp.dot(value_grad.astype(jnp.bfloat16), w_value.T, preferred_element_type=jnp.float32)
    grad_source = norm_back(source, source_gain, pulled_source).astype(jnp.bfloat16)
    pulled_target = jnp.dot(query_grad_rows, w_query.T, preferred_element_type=jnp.float32)
    grad_target = norm_back(target, target_gain, pulled_target).astype(jnp.bfloat16)
    grad_out_w = jnp.dot(attended_rows.T, cotangent, preferred_element_type=jnp.float32).astype(jnp.bfloat16)
    return (grad_target, grad_source, grad_out_w)
```

```python
import functools
import math

import jax
import jax.numpy as jnp
from jax import lax
from jax.experimental import pallas as pl
from jax.experimental.pallas import tpu as pltpu
from jax.sharding import Mesh
from jax.sharding import PartitionSpec as P

HEAD = 128
NORM_EPS = 1e-06
INV_ROOT = HEAD ** (-0.5)
LOG2E = math.log2(math.e)
F32, BF16 = jnp.float32, jnp.bfloat16
NN = (((1,), (0,)), ((), ()))
NT = (((1,), (1,)), ((), ()))
TN = (((0,), (0,)), ((), ()))
SHAPE = {"y": 4, "x": 4, "c": 2}


def dot(a, b, dims):
    return lax.dot_general(a, b, dims, preferred_element_type=F32)


def norm_rows(src, dst, gain):
    rows, step = src.shape[0], 16

    def one(k, carry):
        at = pl.ds(pl.multiple_of(k * step, step), step)
        v = src[at, :].astype(F32)
        r = lax.rsqrt(jnp.mean(v * v, axis=1, keepdims=True) + NORM_EPS)
        dst[at, :] = (v * r * gain[...]).astype(BF16)
        return carry

    lax.fori_loop(0, rows // step, one, 0)


def norm_back(rows, gain, upstream):
    r = lax.rsqrt(jnp.mean(rows * rows, axis=1, keepdims=True) + NORM_EPS)
    unit = rows * r
    pulled = upstream * gain
    return (r * (pulled - unit * jnp.mean(pulled * unit, axis=1, keepdims=True))).astype(BF16)


def wait_bytes(ref, sem):
    pltpu.make_async_copy(ref, ref, sem).wait()


def kernel(
    dims, tgt_h, src_h, cot_h, tg_h, sg_h, wq_h, wk_h, wv_h, wo_h,
    gt_o, gs_o, go_o,
    srcb, swin, sn, tgtb, twin, tn, cotb, tgb, sgb, wqb, wkv, wob,
    kv, qg, est, pgt, ds_b, pr_b, stat, gqt, att,
    ys, yr, gkv, ps, pr, xs, xr, xown, kvs, zk, zr,
    pmat, tpo, tpr, tmine, ts, tr, gos, gor,
    ld, kv_r, kvp_r, qg_r, st_r, y_r, ps_r, x_r, zk_r, tp_r, t_r, go_r,
    kv_s, kvp_s, qg_s, st_s, y_s, ps_s, x_s, zk_s, tp_s, t_s, go_s,
):
    ny, nx, nz, gsz, rt, rs, win = dims
    ns = ny * nx
    y, x, z, c = (lax.axis_index(a) for a in ("y", "x", "z", "c"))
    o = 1 - c
    s_me = y * nx + x
    half = kv.shape[2]
    rows = tgtb.shape[0]
    width = tgtb.shape[1]

    barrier = pltpu.get_barrier_semaphore()
    peers = [{"c": o}]
    for dy in range(ny):
        for dx in range(nx):
            if dy or dx:
                peers.append({"y": lax.rem(y + dy, ny), "x": lax.rem(x + dx, nx)})
    for dz in range(1, nz):
        for cc in (c, o):
            peers.append({"z": lax.rem(z + dz, nz), "c": cc})
    for peer in peers:
        pl.semaphore_signal(barrier, inc=1, device_id=peer, device_id_type=pl.DeviceIdType.MESH)

    def load(k, a, b):
        d = pltpu.make_async_copy(a, b, ld.at[k])
        d.start()
        return d

    t_me = 2 * z + c
    w0 = pl.multiple_of(lax.div(rs * t_me, 8) * 8, 8)
    l_src = load(0, src_h.at[pl.ds(pl.multiple_of(c * half, half), half), :], srcb)
    l_sg = load(1, sg_h, sgb)
    l_wk = load(2, wk_h, wkv.at[:, pl.ds(0, HEAD)])
    l_wv = load(3, wv_h, wkv.at[:, pl.ds(HEAD, HEAD)])
    l_tgt = load(4, tgt_h, tgtb)
    l_tg = load(5, tg_h, tgb)
    l_wq = load(6, wq_h, wqb)
    l_cot = load(7, cot_h, cotb)
    l_wo = load(8, wo_h, wob)
    l_swin = load(9, src_h.at[pl.ds(w0, win), :], swin)
    l_twin = load(10, tgt_h.at[pl.ds(pl.multiple_of(2 * rt * z, 2 * rt), 2 * rt), :], twin)

    def send(a, b, s_sem, r_sem, to):
        d = pltpu.make_async_remote_copy(
            src_ref=a, dst_ref=b, send_sem=s_sem, recv_sem=r_sem,
            device_id=to, device_id_type=pl.DeviceIdType.MESH,
        )
        d.start()
        return d

    l_src.wait()
    l_sg.wait()
    norm_rows(srcb, sn, sgb)
    l_wk.wait()
    l_wv.wait()
    kv[0, c] = dot(sn[...], wkv[...], NN).astype(BF16)
    pl.semaphore_wait(barrier, len(peers))
    sends = []
    for d in range(1, nx):
        sends.append(send(kv.at[0, c], kv.at[d, c], kv_s.at[d], kv_r.at[d], {"x": lax.rem(x + d, nx)}))
    sends.append(send(kv.at[0, c], kv.at[0, c], kvp_s.at[0], kvp_r.at[0], {"c": o}))

    l_tgt.wait()
    l_tg.wait()
    norm_rows(tgtb, tn, tgb)
    l_wq.wait()
    qg[0, :, pl.ds(0, HEAD)] = dot(tn[...], wqb[...], NN).astype(BF16)
    l_cot.wait()
    l_wo.wait()
    qg[0, :, pl.ds(HEAD, HEAD)] = dot(cotb[...], wob[...], NT).astype(BF16)
    for d in range(1, ny):
        sends.append(send(qg.at[0], qg.at[d], qg_s.at[d], qg_r.at[d], {"y": lax.rem(y + d, ny)}))

    for d in range(1, ny):
        wait_bytes(qg.at[d], qg_r.at[d])
    q_all = qg[:, :, pl.ds(0, HEAD)].reshape(ny * rows, HEAD)
    g_all = qg[:, :, pl.ds(HEAD, HEAD)].reshape(ny * rows, HEAD)
    tot = jnp.zeros((1, ny * rows), F32)
    tilt = jnp.zeros((1, ny * rows), F32)

    def unit(d, h, tot, tilt):
        e = jnp.exp2(dot(kv[d, h, :, pl.ds(0, HEAD)], q_all, NT) * (INV_ROOT * LOG2E))
        g = dot(kv[d, h, :, pl.ds(HEAD, HEAD)], g_all, NT)
        est[d, h] = e
        pgt[d, h] = g
        return tot + jnp.sum(e, axis=0, keepdims=True), tilt + jnp.sum(e * g, axis=0, keepdims=True)

    tot, tilt = unit(0, c, tot, tilt)
    for d in range(1, nx):
        wait_bytes(kv.at[d, c], kv_r.at[d])
        sends.append(send(kv.at[d, c], kv.at[d, c], kvp_s.at[d], kvp_r.at[d], {"c": o}))
        wait_bytes(kv.at[d - 1, o], kvp_r.at[d - 1])
        tot, tilt = unit(d - 1, o, tot, tilt)
        tot, tilt = unit(d, c, tot, tilt)
    wait_bytes(kv.at[nx - 1, o], kvp_r.at[nx - 1])
    tot, tilt = unit(nx - 1, o, tot, tilt)

    for e in range(ny):
        stat[0, e, 0:1, :] = tot[:, e * rows:(e + 1) * rows]
        stat[0, e, 1:2, :] = tilt[:, e * rows:(e + 1) * rows]
    for d in range(1, ny):
        sends.append(send(stat.at[0], stat.at[d], st_s.at[d], st_r.at[d], {"y": lax.rem(y + d, ny)}))
    for d in range(1, ny):
        wait_bytes(stat.at[d], st_r.at[d])
    tots, deltas = [], []
    for e in range(ny):
        both = stat[0, e]
        for d in range(1, ny):
            both = both + stat[d, (e - d) % ny]
        tots.append(1.0 / both[0:1, :])
        deltas.append(both[1:2, :] / both[0:1, :])
    inv_total = jnp.concatenate(tots, axis=1)
    delta = jnp.concatenate(deltas, axis=1)

    gq_sum, at_sum = None, None
    for d in range(nx):
        for h in range(2):
            p = est[d, h] * inv_total
            dsv = (p * (pgt[d, h] - delta)).astype(BF16)
            p = p.astype(BF16)
            pr_b[d, h] = p
            ds_b[d, h] = dsv
            gq_one = dot(kv[d, h, :, pl.ds(0, HEAD)], dsv, TN)
            at_one = dot(kv[d, h, :, pl.ds(HEAD, HEAD)], p, TN)
            gq_sum = gq_one if gq_sum is None else gq_sum + gq_one
            at_sum = at_one if at_sum is None else at_sum + at_one
    gqt[...] = gq_sum[:, 0:rows]
    att[...] = at_sum[:, 0:rows]
    for e in range(1, ny):
        ys[e, 0] = gq_sum[:, e * rows:(e + 1) * rows].astype(BF16)
        ys[e, 1] = at_sum[:, e * rows:(e + 1) * rows].astype(BF16)
        sends.append(send(ys.at[e], yr.at[e], y_s.at[e], y_r.at[e], {"y": lax.rem(y + ny - e, ny)}))

    order = [d for d in (2, 1, 3, 0) if d < nx]
    for d in order:
        for h in range(2):
            at = pl.ds(h * half, half)
            gkv[0, d, at, :] = dot(ds_b[d, h], q_all, NN) * INV_ROOT
            gkv[1, d, at, :] = dot(pr_b[d, h], g_all, NN)
        ps[d] = gkv[o, d].astype(BF16)
        sends.append(send(ps.at[d], pr.at[d], ps_s.at[d], ps_r.at[d], {"c": o}))
    for d in order:
        wait_bytes(pr.at[d], ps_r.at[d])
        mine = gkv[c, d] + pr[d].astype(F32)
        if d:
            xs[d] = mine.astype(BF16)
            sends.append(send(xs.at[d], xr.at[d], x_s.at[d], x_r.at[d], {"x": lax.rem(x + nx - d, nx)}))
        else:
            xown[...] = mine

    for e in range(1, ny):
        wait_bytes(yr.at[e], y_r.at[e])
    gq = gqt[...]
    av = att[...]
    for e in range(1, ny):
        gq = gq + yr[e, 0].astype(F32)
        av = av + yr[e, 1].astype(F32)
    gq = (gq * INV_ROOT).T.astype(BF16)
    pmat[...] = dot(gq, wqb[...], NT)
    for k in range(nz):
        a = pmat[pl.ds(2 * rt * k, rt), :]
        b = pmat[pl.ds(2 * rt * k + rt, rt), :]
        tmine[k] = jnp.where(c == 0, a, b)
        tpo[k] = jnp.where(c == 0, b, a).astype(BF16)
    sends.append(send(tpo, tpr, tp_s, tp_r, {"c": o}))
    go = dot(av.astype(BF16), cotb[...], NN)
    wc = width // ns
    for k in range(ns):
        gos[k] = go[:, k * wc:(k + 1) * wc].astype(BF16)
    for dy in (2, 1, 3, 0):
        for dx in (2, 1, 3, 0):
            if dy < ny and dx < nx and (dy or dx):
                py, px = lax.rem(y + dy, ny), lax.rem(x + dx, nx)
                send(gos.at[py * nx + px], gor.at[s_me], go_s, go_r, {"y": py, "x": px})
    wait_bytes(tpr, tp_r)
    ts[...] = (tmine[...] + tpr[...].astype(F32)).astype(BF16)
    far = sorted(range(1, nz), key=lambda k: -min(k, nz - k))
    for dz in far:
        pz = lax.rem(z + dz, nz)
        send(ts.at[pz], tr.at[z], t_s, t_r, {"z": pz})

    ksum = xown[...]
    for d in range(1, nx):
        wait_bytes(xr.at[d], x_r.at[d])
        ksum = ksum + xr[d].astype(F32)
    kvs[...] = ksum
    for k in range(nz):
        for cc in range(2):
            zk[2 * k + cc] = kvs[pl.ds(2 * rs * k + rs * cc, rs), :].astype(BF16)
    for dz in far:
        pz = lax.rem(z + dz, nz)
        for cc in (c, o):
            send(zk.at[2 * pz + cc], zr.at[t_me], zk_s, zk_r, {"z": pz, "c": cc})
    send(zk.at[2 * z + o], zr.at[t_me], zk_s, zk_r, {"c": o})
    zr[t_me] = zk[t_me]
    gor[s_me] = gos[s_me]
    tr[z] = ts[z]

    l_twin.wait()
    wait_bytes(tr.at[pl.ds(0, nz - 1)], t_r)
    up = jnp.sum(tr[...].astype(F32), axis=0)
    tw = twin[...].astype(F32)
    tw = jnp.where(c == 0, tw[0:rt, :], tw[rt:2 * rt, :])
    gt_o[...] = norm_back(tw, tgb[...], up)

    wait_bytes(gor.at[pl.ds(0, ns - 1)], go_r)
    go_o[...] = jnp.sum(gor[...].astype(F32), axis=0).astype(BF16)

    l_swin.wait()
    row_at = lax.broadcasted_iota(jnp.int32, (rs, win), 0) + (rs * t_me - w0)
    pick = (lax.broadcasted_iota(jnp.int32, (rs, win), 1) == row_at).astype(F32).astype(BF16)
    sw = dot(pick, swin[...], NN)
    wait_bytes(zr.at[pl.ds(0, 2 * nz - 1)], zk_r)
    both = [zr[0].astype(F32), zr[1].astype(F32)]
    for k in range(2, 2 * nz):
        both[k % 2] = both[k % 2] + zr[k].astype(F32)
    both = jnp.concatenate(both, axis=1).astype(BF16)
    gs_o[...] = norm_back(sw, sgb[...], dot(both, wkv[...], NT))

    for d in sends:
        d.wait_send()
    wait_bytes(gos.at[pl.ds(0, ns - 1)], go_s)
    wait_bytes(ts.at[pl.ds(0, nz - 1)], t_s)
    wait_bytes(zk.at[pl.ds(0, 2 * nz - 1)], zk_s)


def on_device(shape, target, source, cotangent, target_gain, source_gain, w_query, w_key, w_value, w_out):
    ny, nx, nz = shape
    rows, width = target.shape
    srows = source.shape[0]
    half = srows // 2
    rt, rs = rows // (2 * nz), srows // (2 * nz)
    win = rs if rs % 8 == 0 else rs + 4
    ns = ny * nx
    wide = ny * rows
    vm = pltpu.VMEM
    sem = pltpu.SemaphoreType.DMA
    scratch = [
        vm((half, width), BF16), vm((win, width), BF16), vm((half, width), BF16),
        vm((rows, width), BF16), vm((2 * rt, width), BF16), vm((rows, width), BF16),
        vm((rows, width), BF16), vm((1, width), F32), vm((1, width), F32),
        vm((width, HEAD), BF16), vm((width, 2 * HEAD), BF16), vm((HEAD, width), BF16),
        vm((nx, 2, half, 2 * HEAD), BF16), vm((ny, rows, 2 * HEAD), BF16),
        vm((nx, 2, half, wide), F32), vm((nx, 2, half, wide), F32),
        vm((nx, 2, half, wide), BF16), vm((nx, 2, half, wide), BF16),
        vm((ny, ny, 2, rows), F32), vm((HEAD, rows), F32), vm((HEAD, rows), F32),
        vm((ny, 2, HEAD, rows), BF16), vm((ny, 2, HEAD, rows), BF16),
        vm((2, nx, srows, HEAD), F32), vm((nx, srows, HEAD), BF16), vm((nx, srows, HEAD), BF16),
        vm((nx, srows, HEAD), BF16), vm((nx, srows, HEAD), BF16), vm((srows, HEAD), F32),
        vm((srows, HEAD), F32), vm((2 * nz, rs, HEAD), BF16), vm((2 * nz, rs, HEAD), BF16),
        vm((rows, width), F32), vm((nz, rt, width), BF16), vm((nz, rt, width), BF16),
        vm((nz, rt, width), F32), vm((nz, rt, width), BF16), vm((nz, rt, width), BF16),
        vm((ns, HEAD, width // ns), BF16), vm((ns, HEAD, width // ns), BF16),
        sem((11,)), sem((nx,)), sem((nx,)), sem((ny,)), sem((ny,)), sem((ny,)), sem((nx,)), sem((nx,)),
        sem, sem, sem, sem,
        sem((nx,)), sem((nx,)), sem((ny,)), sem((ny,)), sem((ny,)), sem((nx,)), sem((nx,)),
        sem, sem, sem, sem,
    ]
    any_spec = pl.BlockSpec(memory_space=pl.ANY)
    vm_spec = pl.BlockSpec(memory_space=pltpu.VMEM)
    return pl.pallas_call(
        functools.partial(kernel, (ny, nx, nz, 0, rt, rs, win)),
        out_shape=(
            jax.ShapeDtypeStruct((rt, width), BF16),
            jax.ShapeDtypeStruct((rs, width), BF16),
            jax.ShapeDtypeStruct((HEAD, width // ns), BF16),
        ),
        in_specs=[any_spec] * 9,
        out_specs=(vm_spec,) * 3,
        scratch_shapes=scratch,
        compiler_params=pltpu.CompilerParams(
            collective_id=0, has_side_effects=True, vmem_limit_bytes=67043328
        ),
    )(
        target, source, cotangent, target_gain.reshape(1, width), source_gain.reshape(1, width),
        w_query, w_key, w_value, w_out,
    )


def solution(mesh, ny=4, nx=4):
    nz = mesh.shape["tp"] // 2
    split = Mesh(mesh.devices.reshape(ny, nx, nz, 2), ("y", "x", "z", "c"))
    sp, tp, every = ("y", "x"), ("z", "c"), ("y", "x", "z", "c")
    in_specs = (P(sp, None), P(sp, None), P(sp, None), P(), P(), P(None, tp), P(), P(), P(tp, None))
    out_specs = (P(every, None), P(every, None), P(tp, sp))
    return jax.shard_map(
        functools.partial(on_device, (ny, nx, nz)),
        mesh=split, in_specs=in_specs, out_specs=out_specs, check_vma=False,
    )
```

```python
import functools
import math

import jax
import jax.numpy as jnp
from jax import lax
from jax.experimental import pallas as pl
from jax.experimental.pallas import tpu as pltpu
from jax.sharding import Mesh
from jax.sharding import PartitionSpec as P

HEAD = 128
NORM_EPS = 1e-06
INV_ROOT = HEAD ** (-0.5)
LOG2E = math.log2(math.e)
F32, BF16 = jnp.float32, jnp.bfloat16
NN = (((1,), (0,)), ((), ()))
NT = (((1,), (1,)), ((), ()))
TN = (((0,), (0,)), ((), ()))
SHAPE = {"y": 4, "x": 4, "c": 2}


def dot(a, b, dims):
    return lax.dot_general(a, b, dims, preferred_element_type=F32)


def norm_rows(src, dst, gain):
    rows, step = src.shape[0], 16

    def one(k, carry):
        at = pl.ds(pl.multiple_of(k * step, step), step)
        v = src[at, :].astype(F32)
        r = lax.rsqrt(jnp.mean(v * v, axis=1, keepdims=True) + NORM_EPS)
        dst[at, :] = (v * r * gain[...]).astype(BF16)
        return carry

    lax.fori_loop(0, rows // step, one, 0, unroll=4)


def norm_back(rows, gain, upstream):
    r = lax.rsqrt(jnp.mean(rows * rows, axis=1, keepdims=True) + NORM_EPS)
    unit = rows * r
    pulled = upstream * gain
    return (r * (pulled - unit * jnp.mean(pulled * unit, axis=1, keepdims=True))).astype(BF16)


def wait_bytes(ref, sem):
    pltpu.make_async_copy(ref, ref, sem).wait()


def kernel(
    dims, tgt_h, src_h, cot_h, tg_h, sg_h, wq_h, wk_h, wv_h, wo_h,
    gt_o, gs_o, go_o,
    srcb, swin, sn, tgtb, twin, tn, cotb, tgb, sgb, wkv, wob,
    kv, qg, est, pgt, e_b, t_b, stat, aw, tk,
    ys, yr, gkv, ps, pr, xs, xr, xown, kvs, zk, zr,
    wq4, gqo, gqi, pmat, ts, tr, gos, gor,
    ld, kv_r, kvp_r, qg_r, st_r, y_r, ps_r, x_r, zk_r, wq_r, gq_r, t_r, go_r,
    kv_s, kvp_s, qg_s, st_s, y_s, ps_s, x_s, zk_s, wq_s, gq_s, t_s, go_s,
    up_1, up_2, up_4,
):
    ny, nx, nz, gsz, rt, rs, win = dims
    ns = ny * nx
    y, x, z, c = (lax.axis_index(a) for a in ("y", "x", "z", "c"))
    o = 1 - c
    s_me = y * nx + x
    zo = z + 1 - 2 * lax.rem(z, 2)
    zf = lax.rem(z - 1 + 2 * lax.rem(z, 2) + nz, nz)
    mem = 2 * lax.rem(z, 2) + c
    half = kv.shape[2]
    rows = tgtb.shape[0]
    width = tgtb.shape[1]

    barrier = pltpu.get_barrier_semaphore()

    def signal(sem, to):
        pl.semaphore_signal(sem, inc=1, device_id=to, device_id_type=pl.DeviceIdType.MESH)

    def beside(k):
        return [lax.rem(z + k, nz), lax.rem(z + nz - k, nz)] if 2 * k < nz else [lax.rem(z + k, nz)]

    peers = [{"c": o}]
    for dy in range(ny):
        for dx in range(nx):
            if dy or dx:
                peers.append({"y": lax.rem(y + dy, ny), "x": lax.rem(x + dx, nx)})
    for dy in range(ny):
        py = lax.rem(y + dy, ny)
        peers.extend([{"y": py, "z": zo, "c": c}, {"y": py, "z": zo, "c": o}])
        if dy:
            peers.append({"y": py, "c": o})
    if nz > 2:
        peers.extend([{"z": zf, "c": c}, {"z": zf, "c": o}])
    for peer in peers:
        signal(barrier, peer)

    def load(k, a, b):
        d = pltpu.make_async_copy(a, b, ld.at[k])
        d.start()
        return d

    t_me = 2 * z + c
    w0 = pl.multiple_of(lax.div(rs * t_me, 8) * 8, 8)
    l_tgt = load(4, tgt_h, tgtb)
    l_tg = load(5, tg_h, tgb)
    l_wq = load(6, wq_h, wq4.at[mem])
    l_cot = load(7, cot_h, cotb)
    l_wo = load(8, wo_h, wob)
    l_src = load(0, src_h.at[pl.ds(pl.multiple_of(c * half, half), half), :], srcb)
    l_sg = load(1, sg_h, sgb)
    l_wk = load(2, wk_h, wkv.at[:, pl.ds(0, HEAD)])
    l_wv = load(3, wv_h, wkv.at[:, pl.ds(HEAD, HEAD)])
    l_swin = load(9, src_h.at[pl.ds(w0, win), :], swin)
    l_twin = load(10, tgt_h.at[pl.ds(pl.multiple_of(2 * rt * z, 2 * rt), 2 * rt), :], twin)

    def send(a, b, s_sem, r_sem, to):
        d = pltpu.make_async_remote_copy(
            src_ref=a, dst_ref=b, send_sem=s_sem, recv_sem=r_sem,
            device_id=to, device_id_type=pl.DeviceIdType.MESH,
        )
        d.start()
        return d

    l_tgt.wait()
    l_tg.wait()
    norm_rows(tgtb, tn, tgb)
    l_wq.wait()
    qg[0, :, pl.ds(0, HEAD)] = dot(tn[...], wq4[mem], NN).astype(BF16)
    l_cot.wait()
    l_wo.wait()
    qg[0, :, pl.ds(HEAD, HEAD)] = dot(cotb[...], wob[...], NT).astype(BF16)
    pl.semaphore_wait(barrier, len(peers))
    sends = []
    x_order = [d for d in (2, 1, 3) if d < nx]
    y_order = [d for d in (2, 1, 3) if d < ny]
    for d in y_order:
        sends.append(send(qg.at[0], qg.at[d], qg_s.at[d], qg_r.at[d], {"y": lax.rem(y + d, ny)}))
    for pz in beside(1):
        signal(up_1, {"z": pz})
    sends.append(send(wq4.at[mem], wq4.at[mem], wq_s.at[0], wq_r.at[0], {"z": zo}))
    sends.append(send(wq4.at[mem], wq4.at[mem], wq_s.at[1], wq_r.at[1], {"c": o}))

    l_src.wait()
    l_sg.wait()
    norm_rows(srcb, sn, sgb)
    l_wk.wait()
    l_wv.wait()
    kv[0, c] = dot(sn[...], wkv[...], NN).astype(BF16)
    for d in x_order:
        sends.append(send(kv.at[0, c], kv.at[d, c], kv_s.at[d], kv_r.at[d], {"x": lax.rem(x + d, nx)}))
    sends.append(send(kv.at[0, c], kv.at[0, c], kvp_s.at[0], kvp_r.at[0], {"c": o}))
    pl.semaphore_wait(up_1, len(beside(1)))
    for pz in beside(2):
        signal(up_2, {"z": pz})

    for d in range(1, ny):
        wait_bytes(qg.at[d], qg_r.at[d])
    pl.semaphore_wait(up_2, len(beside(2)))
    for pz in beside(4):
        signal(up_4, {"z": pz})
    q_all = qg[:, :, pl.ds(0, HEAD)].reshape(ny * rows, HEAD)
    g_all = qg[:, :, pl.ds(HEAD, HEAD)].reshape(ny * rows, HEAD)
    tot = jnp.zeros((1, ny * rows), F32)
    tilt = jnp.zeros((1, ny * rows), F32)

    def unit(d, h, tot, tilt):
        key, val = kv[d, h, :, pl.ds(0, HEAD)], kv[d, h, :, pl.ds(HEAD, HEAD)]
        e = jnp.exp2(dot(key, q_all, NT) * (INV_ROOT * LOG2E))
        g = dot(val, g_all, NT)
        t = e * g
        est[d, h] = e
        pgt[d, h] = g
        e_b[d, h] = e.astype(BF16)
        t_b[d, h] = t.astype(BF16)
        return tot + jnp.sum(e, axis=0, keepdims=True), tilt + jnp.sum(t, axis=0, keepdims=True)

    def unit_sums(d, h, first):
        both = dot(kv[d, h], e_b[d, h], TN)
        one = dot(kv[d, h, :, pl.ds(0, HEAD)], t_b[d, h], TN)
        aw[...] = both if first else aw[...] + both
        tk[...] = one if first else tk[...] + one

    x_seen = [d for d in (1, 3, 2) if d < nx]
    tot, tilt = unit(0, c, tot, tilt)
    unit_sums(0, c, True)
    before = 0
    for d in x_seen:
        wait_bytes(kv.at[d, c], kv_r.at[d])
        sends.append(send(kv.at[d, c], kv.at[d, c], kvp_s.at[d], kvp_r.at[d], {"c": o}))
        wait_bytes(kv.at[before, o], kvp_r.at[before])
        tot, tilt = unit(before, o, tot, tilt)
        unit_sums(before, o, False)
        tot, tilt = unit(d, c, tot, tilt)
        if d != x_seen[-1]:
            unit_sums(d, c, False)
        before = d
    wait_bytes(kv.at[before, o], kvp_r.at[before])
    tot, tilt = unit(before, o, tot, tilt)

    for e in range(ny):
        stat[0, e, 0:1, :] = tot[:, e * rows:(e + 1) * rows]
        stat[0, e, 1:2, :] = tilt[:, e * rows:(e + 1) * rows]
    for d in y_order:
        sends.append(send(stat.at[0], stat.at[d], st_s.at[d], st_r.at[d], {"y": lax.rem(y + d, ny)}))
    unit_sums(before, c, False)
    unit_sums(before, o, False)
    for e in y_order:
        ys[e] = aw[pl.ds(HEAD, HEAD), pl.ds(e * rows, rows)].astype(BF16)
        sends.append(send(ys.at[e], yr.at[e], y_s.at[e], y_r.at[e], {"y": lax.rem(y + ny - e, ny)}))
    for d in range(1, ny):
        wait_bytes(stat.at[d], st_r.at[d])
    tots, deltas = [], []
    for e in range(ny):
        both = stat[0, e]
        for d in range(1, ny):
            both = both + stat[d, (e - d) % ny]
        tots.append(1.0 / both[0:1, :])
        deltas.append(both[1:2, :] / both[0:1, :])
    inv_total = jnp.concatenate(tots, axis=1)
    delta = jnp.concatenate(deltas, axis=1)

    gq = ((tk[...] - delta * aw[pl.ds(0, HEAD), :]) * (inv_total * INV_ROOT)).T.astype(BF16)
    quarter = rows // 4
    for e in range(ny):
        for k in range(4):
            gqo[4 * e + k] = gq[e * rows + k * quarter:e * rows + (k + 1) * quarter, :]
    for e in y_order + [0]:
        py = lax.rem(y + ny - e, ny)
        for step in (2, 3, 1, 0):
            if e or step:
                pz = zo if step > 1 else z
                pc = o if step % 2 else c
                to = 2 * lax.rem(pz, 2) + pc
                send(gqo.at[4 * e + to], gqi.at[4 * e + mem], gq_s, gq_r, {"y": py, "z": pz, "c": pc})
    gqi[mem] = gqo[mem]
    scale = jnp.broadcast_to(inv_total, (8, ny * rows)).T[:, 0:1]
    q_div = (q_all.astype(F32) * scale).astype(BF16)
    g_div = (g_all.astype(F32) * scale).astype(BF16)
    order = [d for d in (2, 1, 3, 0) if d < nx]
    for d in order:
        for h in range(2):
            at = pl.ds(h * half, half)
            dsv = (est[d, h] * (pgt[d, h] - delta)).astype(BF16)
            gkv[0, d, at, :] = dot(dsv, q_div, NN) * INV_ROOT
            gkv[1, d, at, :] = dot(e_b[d, h], g_div, NN)
        ps[d] = gkv[o, d].astype(BF16)
        sends.append(send(ps.at[d], pr.at[d], ps_s.at[d], ps_r.at[d], {"c": o}))
    for d in order:
        wait_bytes(pr.at[d], ps_r.at[d])
        mine = gkv[c, d] + pr[d].astype(F32)
        if d:
            xs[d] = mine.astype(BF16)
            sends.append(send(xs.at[d], xr.at[d], x_s.at[d], x_r.at[d], {"x": lax.rem(x + nx - d, nx)}))
        else:
            xown[...] = mine

    wait_bytes(wq4.at[0], wq_r.at[0])
    mem_z = 2 * lax.rem(zo, 2) + c
    sends.append(send(wq4.at[mem_z], wq4.at[mem_z], wq_s.at[2], wq_r.at[2], {"c": o}))
    wait_bytes(gqi.at[pl.ds(0, 4 * ny - 1)], gq_r)
    wait_bytes(wq4.at[0], wq_r.at[1])
    wait_bytes(wq4.at[0], wq_r.at[2])
    up = None
    for k in range(4):
        one = gqi[k].astype(F32)
        for e in range(1, ny):
            one = one + gqi[4 * e + k].astype(F32)
        one = dot(one.astype(BF16), wq4[k], NT)
        up = one if up is None else up + one
    pmat[...] = up
    pieces = quarter // rt
    for k in range(pieces):
        ts[k] = pmat[pl.ds(rt * k, rt), :].astype(BF16)
    pl.semaphore_wait(up_4, len(beside(4)))
    pair = lax.div(z, 2)
    per = pieces // 2
    for k in range(pieces):
        pz, pc = per * mem + k // 2, k % 2
        mine = jnp.logical_and(pz == z, pc == c)

        @pl.when(jnp.logical_not(mine))
        def _():
            send(ts.at[k], tr.at[pair], t_s, t_r, {"z": pz, "c": pc})

        @pl.when(mine)
        def _():
            tr[pair] = ts[k]

    for e in range(1, ny):
        wait_bytes(yr.at[e], y_r.at[e])
    av = aw[pl.ds(HEAD, HEAD), pl.ds(0, rows)]
    for e in range(1, ny):
        av = av + yr[e].astype(F32)
    go = dot((av * tots[0]).astype(BF16), cotb[...], NN)
    wc = width // ns
    for k in range(ns):
        gos[k] = go[:, k * wc:(k + 1) * wc].astype(BF16)
    for dy in (2, 1, 3, 0):
        for dx in (2, 1, 3, 0):
            if dy < ny and dx < nx and (dy or dx):
                py, px = lax.rem(y + dy, ny), lax.rem(x + dx, nx)
                send(gos.at[py * nx + px], gor.at[s_me], go_s, go_r, {"y": py, "x": px})
    far = sorted(range(1, nz), key=lambda k: -min(k, nz - k))

    ksum = xown[...]
    for d in range(1, nx):
        wait_bytes(xr.at[d], x_r.at[d])
        ksum = ksum + xr[d].astype(F32)
    kvs[...] = ksum
    for k in range(nz):
        for cc in range(2):
            zk[2 * k + cc] = kvs[pl.ds(2 * rs * k + rs * cc, rs), :].astype(BF16)
    for dz in far:
        pz = lax.rem(z + dz, nz)
        for cc in (c, o):
            send(zk.at[2 * pz + cc], zr.at[t_me], zk_s, zk_r, {"z": pz, "c": cc})
    send(zk.at[2 * z + o], zr.at[t_me], zk_s, zk_r, {"c": o})
    zr[t_me] = zk[t_me]
    gor[s_me] = gos[s_me]

    l_swin.wait()
    row_at = lax.broadcasted_iota(jnp.int32, (rs, win), 0) + (rs * t_me - w0)
    pick = (lax.broadcasted_iota(jnp.int32, (rs, win), 1) == row_at).astype(F32).astype(BF16)
    sw = dot(pick, swin[...], NN)
    l_twin.wait()
    own_piece = mem == lax.div(z, per)

    @pl.when(own_piece)
    def _():
        wait_bytes(tr.at[pl.ds(0, nz // 2 - 1)], t_r)
        wait_bytes(ts.at[pl.ds(0, pieces - 1)], t_s)

    @pl.when(jnp.logical_not(own_piece))
    def _():
        wait_bytes(tr, t_r)
        wait_bytes(ts, t_s)

    up = jnp.sum(tr[...].astype(F32), axis=0)
    tw = twin[...].astype(F32)
    tw = jnp.where(c == 0, tw[0:rt, :], tw[rt:2 * rt, :])
    gt_o[...] = norm_back(tw, tgb[...], up)

    wait_bytes(gor.at[pl.ds(0, ns - 1)], go_r)
    go_o[...] = jnp.sum(gor[...].astype(F32), axis=0).astype(BF16)

    wait_bytes(zr.at[pl.ds(0, 2 * nz - 1)], zk_r)
    both = [zr[0].astype(F32), zr[1].astype(F32)]
    for k in range(2, 2 * nz):
        both[k % 2] = both[k % 2] + zr[k].astype(F32)
    both = jnp.concatenate(both, axis=1).astype(BF16)
    gs_o[...] = norm_back(sw, sgb[...], dot(both, wkv[...], NT))

    for d in sends:
        d.wait_send()
    wait_bytes(gos.at[pl.ds(0, ns - 1)], go_s)
    wait_bytes(gqo.at[pl.ds(0, 4 * ny - 1)], gq_s)
    wait_bytes(zk.at[pl.ds(0, 2 * nz - 1)], zk_s)


def write_out(a, b, c, a_o, b_o, c_o, sems):
    copies = [pltpu.make_async_copy(i, j, sems.at[k]) for k, (i, j) in enumerate(((a, a_o), (b, b_o), (c, c_o)))]
    for one in copies:
        one.start()
    for one in copies:
        one.wait()


def on_device(shape, target, source, cotangent, target_gain, source_gain, w_query, w_key, w_value, w_out):
    ny, nx, nz = shape
    rows, width = target.shape
    srows = source.shape[0]
    half = srows // 2
    rt, rs = rows // (2 * nz), srows // (2 * nz)
    win = rs if rs % 8 == 0 else rs + 4
    ns = ny * nx
    wide = ny * rows
    vm = pltpu.VMEM
    sem = pltpu.SemaphoreType.DMA
    scratch = [
        vm((half, width), BF16), vm((win, width), BF16), vm((half, width), BF16),
        vm((rows, width), BF16), vm((2 * rt, width), BF16), vm((rows, width), BF16),
        vm((rows, width), BF16), vm((1, width), F32), vm((1, width), F32),
        vm((width, 2 * HEAD), BF16), vm((HEAD, width), BF16),
        vm((nx, 2, half, 2 * HEAD), BF16), vm((ny, rows, 2 * HEAD), BF16),
        vm((nx, 2, half, wide), F32), vm((nx, 2, half, wide), F32),
        vm((nx, 2, half, wide), BF16), vm((nx, 2, half, wide), BF16),
        vm((ny, ny, 2, rows), F32), vm((2 * HEAD, wide), F32), vm((HEAD, wide), F32),
        vm((ny, HEAD, rows), BF16), vm((ny, HEAD, rows), BF16),
        vm((2, nx, srows, HEAD), F32), vm((nx, srows, HEAD), BF16), vm((nx, srows, HEAD), BF16),
        vm((nx, srows, HEAD), BF16), vm((nx, srows, HEAD), BF16), vm((srows, HEAD), F32),
        vm((srows, HEAD), F32), vm((2 * nz, rs, HEAD), BF16), vm((2 * nz, rs, HEAD), BF16),
        vm((4, width, HEAD), BF16), vm((4 * ny, rows // 4, HEAD), BF16), vm((4 * ny, rows // 4, HEAD), BF16),
        vm((rows // 4, width), F32), vm((rows // 4 // rt, rt, width), BF16), vm((nz // 2, rt, width), BF16),
        vm((ns, HEAD, width // ns), BF16), vm((ns, HEAD, width // ns), BF16),
        sem((11,)), sem((nx,)), sem((nx,)), sem((ny,)), sem((ny,)), sem((ny,)), sem((nx,)), sem((nx,)),
        sem, sem((3,)), sem, sem, sem,
        sem((nx,)), sem((nx,)), sem((ny,)), sem((ny,)), sem((ny,)), sem((nx,)), sem((nx,)),
        sem, sem((3,)), sem, sem, sem,
        pltpu.SemaphoreType.REGULAR, pltpu.SemaphoreType.REGULAR, pltpu.SemaphoreType.REGULAR,
    ]
    any_spec = pl.BlockSpec(memory_space=pltpu.HBM)
    vm_spec = pl.BlockSpec(memory_space=pltpu.VMEM)
    made = pl.pallas_call(
        functools.partial(kernel, (ny, nx, nz, 0, rt, rs, win)),
        out_shape=(
            vm((rt, width), BF16), vm((rs, width), BF16), vm((HEAD, width // ns), BF16),
        ),
        in_specs=[any_spec] * 9,
        out_specs=(vm_spec,) * 3,
        scratch_shapes=scratch,
        compiler_params=pltpu.CompilerParams(
            collective_id=0, has_side_effects=True, vmem_limit_bytes=56 * 1024 * 1024
        ),
    )(*(pltpu.with_memory_space_constraint(a, pltpu.HBM) for a in (
        target, source, cotangent, target_gain.reshape(1, width), source_gain.reshape(1, width),
        w_query, w_key, w_value, w_out,
    )))
    return pl.pallas_call(
        write_out,
        out_shape=tuple(jax.ShapeDtypeStruct(m.shape, m.dtype) for m in made),
        in_specs=[vm_spec] * 3,
        out_specs=(pl.BlockSpec(memory_space=pltpu.HBM),) * 3,
        scratch_shapes=[sem((3,))],
        compiler_params=pltpu.CompilerParams(vmem_limit_bytes=1024 * 1024),
    )(*made)


def solution(mesh, ny=4, nx=4):
    nz = mesh.shape["tp"] // 2
    split = Mesh(mesh.devices.reshape(ny, nx, nz, 2), ("y", "x", "z", "c"))
    sp, tp, every = ("y", "x"), ("z", "c"), ("y", "x", "z", "c")
    in_specs = (P(sp, None), P(sp, None), P(sp, None), P(), P(), P(None, tp), P(), P(), P(tp, None))
    out_specs = (P(every, None), P(every, None), P(tp, sp))
    return jax.shard_map(
        functools.partial(on_device, (ny, nx, nz)),
        mesh=split, in_specs=in_specs, out_specs=out_specs, check_vma=False,
    )
```

```python
import functools
import math

import jax
import jax.numpy as jnp
from jax import lax
from jax.experimental import pallas as pl
from jax.experimental.pallas import tpu as pltpu
from jax.sharding import Mesh
from jax.sharding import PartitionSpec as P

HEAD = 128
NORM_EPS = 1e-06
INV_ROOT = HEAD ** (-0.5)
LOG2E = math.log2(math.e)
F32, BF16 = jnp.float32, jnp.bfloat16
NN = (((1,), (0,)), ((), ()))
NT = (((1,), (1,)), ((), ()))
TN = (((0,), (0,)), ((), ()))
SHAPE = {"y": 4, "x": 4, "c": 2}


def dot(a, b, dims):
    return lax.dot_general(a, b, dims, preferred_element_type=F32)


def norm_rows(src, dst, gain):
    rows, step = src.shape[0], 16

    def one(k, carry):
        at = pl.ds(pl.multiple_of(k * step, step), step)
        v = src[at, :].astype(F32)
        r = lax.rsqrt(jnp.mean(v * v, axis=1, keepdims=True) + NORM_EPS)
        dst[at, :] = (v * r * gain[...]).astype(BF16)
        return carry

    lax.fori_loop(0, rows // step, one, 0, unroll=4)


def norm_back(rows, gain, upstream):
    r = lax.rsqrt(jnp.mean(rows * rows, axis=1, keepdims=True) + NORM_EPS)
    unit = rows * r
    pulled = upstream * gain
    return (r * (pulled - unit * jnp.mean(pulled * unit, axis=1, keepdims=True))).astype(BF16)


def wait_bytes(ref, sem):
    pltpu.make_async_copy(ref, ref, sem).wait()


def kernel(
    dims, tgt_h, src_h, cot_h, tg_h, sg_h, wq_h, wk_h, wv_h, wo_h,
    gt_o, gs_o, go_o,
    srcb, swin, sn, tgtb, twin, tn, cotb, tgb, sgb, wkv, wob,
    kv, qg, est, pgt, e_b, t_b, stat, aw, tk,
    ys, yr, gkv, ps, pr, xs, xr, xown, zk, zr,
    wq4, gqo, gqi, pmat, ts, tr, gos, gor,
    ld, kv_r, kvp_r, qg_r, st_r, y_r, ps_r, x_r, zk_r, wq_r, gq_r, t_r, go_r,
    kv_s, kvp_s, qg_s, st_s, y_s, ps_s, x_s, zk_s, wq_s, gq_s, t_s, go_s,
    up_1, up_2, up_4,
):
    ny, nx, nz, gsz, rt, rs, win = dims
    ns = ny * nx
    y, x, z, c = (lax.axis_index(a) for a in ("y", "x", "z", "c"))
    o = 1 - c
    s_me = y * nx + x
    zo = z + 1 - 2 * lax.rem(z, 2)
    zf = lax.rem(z - 1 + 2 * lax.rem(z, 2) + nz, nz)
    hz = lax.rem(z, 2)
    mem = 2 * hz + c
    half = kv.shape[2]
    rows = tgtb.shape[0]
    width = tgtb.shape[1]

    barrier = pltpu.get_barrier_semaphore()

    def signal(sem, to):
        pl.semaphore_signal(sem, inc=1, device_id=to, device_id_type=pl.DeviceIdType.MESH)

    def beside(k):
        return [lax.rem(z + k, nz), lax.rem(z + nz - k, nz)] if 2 * k < nz else [lax.rem(z + k, nz)]

    peers = [{"c": o}]
    for dy in range(ny):
        for dx in range(nx):
            if dy or dx:
                peers.append({"y": lax.rem(y + dy, ny), "x": lax.rem(x + dx, nx)})
    for dy in range(ny):
        py = lax.rem(y + dy, ny)
        peers.extend([{"y": py, "z": zo, "c": c}, {"y": py, "z": zo, "c": o}])
        if dy:
            peers.append({"y": py, "c": o})
    for dx in range(1, nx):
        peers.append({"x": lax.rem(x + dx, nx), "z": zo})
    if nz > 2:
        peers.extend([{"z": zf, "c": c}, {"z": zf, "c": o}])
    for peer in peers:
        signal(barrier, peer)

    def load(k, a, b):
        d = pltpu.make_async_copy(a, b, ld.at[k])
        d.start()
        return d

    t_me = 2 * z + c
    w0 = pl.multiple_of(lax.div(rs * t_me, 8) * 8, 8)
    l_tgt = load(4, tgt_h, tgtb)
    l_tg = load(5, tg_h, tgb)
    l_wq = load(6, wq_h, wq4.at[mem])
    l_cot = load(7, cot_h, cotb)
    l_wo = load(8, wo_h, wob)
    l_src = load(0, src_h.at[pl.ds(pl.multiple_of(c * half, half), half), :], srcb)
    l_sg = load(1, sg_h, sgb)
    l_wk = load(2, wk_h, wkv.at[:, pl.ds(0, HEAD)])
    l_wv = load(3, wv_h, wkv.at[:, pl.ds(HEAD, HEAD)])
    l_swin = load(9, src_h.at[pl.ds(w0, win), :], swin)
    l_twin = load(10, tgt_h.at[pl.ds(pl.multiple_of(2 * rt * z, 2 * rt), 2 * rt), :], twin)

    def send(a, b, s_sem, r_sem, to):
        d = pltpu.make_async_remote_copy(
            src_ref=a, dst_ref=b, send_sem=s_sem, recv_sem=r_sem,
            device_id=to, device_id_type=pl.DeviceIdType.MESH,
        )
        d.start()
        return d

    l_tgt.wait()
    l_tg.wait()
    norm_rows(tgtb, tn, tgb)
    l_wq.wait()
    qg[0, :, pl.ds(0, HEAD)] = dot(tn[...], wq4[mem], NN).astype(BF16)
    l_cot.wait()
    l_wo.wait()
    qg[0, :, pl.ds(HEAD, HEAD)] = dot(cotb[...], wob[...], NT).astype(BF16)
    l_src.wait()
    l_sg.wait()
    norm_rows(srcb, sn, sgb)
    l_wk.wait()
    l_wv.wait()
    kv[0, c] = dot(sn[...], wkv[...], NN).astype(BF16)
    pl.semaphore_wait(barrier, len(peers))
    sends = []
    x_order = [d for d in (2, 1, 3) if d < nx]
    y_order = [d for d in (2, 1, 3) if d < ny]
    for d in y_order:
        sends.append(send(qg.at[0], qg.at[d], qg_s.at[d], qg_r.at[d], {"y": lax.rem(y + d, ny)}))
    for pz in beside(1):
        signal(up_1, {"z": pz})
    sends.append(send(wq4.at[mem], wq4.at[mem], wq_s.at[0], wq_r.at[0], {"z": zo}))
    sends.append(send(wq4.at[mem], wq4.at[mem], wq_s.at[1], wq_r.at[1], {"c": o}))
    for d in x_order:
        sends.append(send(kv.at[0, c], kv.at[d, c], kv_s.at[d], kv_r.at[d], {"x": lax.rem(x + d, nx)}))
    sends.append(send(kv.at[0, c], kv.at[0, c], kvp_s.at[0], kvp_r.at[0], {"c": o}))
    pl.semaphore_wait(up_1, len(beside(1)))
    for pz in beside(2):
        signal(up_2, {"z": pz})

    for d in range(1, ny):
        wait_bytes(qg.at[d], qg_r.at[d])
    pl.semaphore_wait(up_2, len(beside(2)))
    for pz in beside(4):
        signal(up_4, {"z": pz})
    q_all = qg[:, :, pl.ds(0, HEAD)].reshape(ny * rows, HEAD)
    g_all = qg[:, :, pl.ds(HEAD, HEAD)].reshape(ny * rows, HEAD)
    tot = jnp.zeros((1, ny * rows), F32)
    tilt = jnp.zeros((1, ny * rows), F32)

    def unit(d, h, tot, tilt):
        key, val = kv[d, h, :, pl.ds(0, HEAD)], kv[d, h, :, pl.ds(HEAD, HEAD)]
        e = jnp.exp2(dot(key, q_all, NT) * (INV_ROOT * LOG2E))
        g = dot(val, g_all, NT)
        t = e * g
        est[d, h] = e
        pgt[d, h] = g
        e_b[d, h] = e.astype(BF16)
        t_b[d, h] = t.astype(BF16)
        return tot + jnp.sum(e, axis=0, keepdims=True), tilt + jnp.sum(t, axis=0, keepdims=True)

    def unit_sums(d, h, first):
        both = dot(kv[d, h], e_b[d, h], TN)
        one = dot(kv[d, h, :, pl.ds(0, HEAD)], t_b[d, h], TN)
        aw[...] = both if first else aw[...] + both
        tk[...] = one if first else tk[...] + one

    x_seen = [d for d in (1, 3, 2) if d < nx]
    tot, tilt = unit(0, c, tot, tilt)
    before = 0
    for d in x_seen:
        wait_bytes(kv.at[d, c], kv_r.at[d])
        sends.append(send(kv.at[d, c], kv.at[d, c], kvp_s.at[d], kvp_r.at[d], {"c": o}))
        wait_bytes(kv.at[before, o], kvp_r.at[before])
        tot, tilt = unit(before, o, tot, tilt)
        tot, tilt = unit(d, c, tot, tilt)
        before = d
    wait_bytes(kv.at[before, o], kvp_r.at[before])
    tot, tilt = unit(before, o, tot, tilt)

    for e in range(ny):
        stat[0, e, 0:1, :] = tot[:, e * rows:(e + 1) * rows]
        stat[0, e, 1:2, :] = tilt[:, e * rows:(e + 1) * rows]
    for d in y_order:
        sends.append(send(stat.at[0], stat.at[d], st_s.at[d], st_r.at[d], {"y": lax.rem(y + d, ny)}))
    for d in range(nx):
        for h in range(2):
            unit_sums(d, h, d + h == 0)
    for e in y_order:
        ys[e] = aw[pl.ds(HEAD, HEAD), pl.ds(e * rows, rows)].astype(BF16)
        sends.append(send(ys.at[e], yr.at[e], y_s.at[e], y_r.at[e], {"y": lax.rem(y + ny - e, ny)}))
    for d in range(1, ny):
        wait_bytes(stat.at[d], st_r.at[d])
    tots, deltas = [], []
    for e in range(ny):
        both = stat[0, e]
        for d in range(1, ny):
            both = both + stat[d, (e - d) % ny]
        tots.append(1.0 / both[0:1, :])
        deltas.append(both[1:2, :] / both[0:1, :])
    inv_total = jnp.concatenate(tots, axis=1)
    delta = jnp.concatenate(deltas, axis=1)

    gq = ((tk[...] - delta * aw[pl.ds(0, HEAD), :]) * (inv_total * INV_ROOT)).T.astype(BF16)
    quarter = rows // 4
    for e in range(ny):
        for k in range(4):
            gqo[4 * e + k] = gq[e * rows + k * quarter:e * rows + (k + 1) * quarter, :]
    for e in y_order + [0]:
        py = lax.rem(y + ny - e, ny)
        for step in (2, 3, 1, 0):
            if e or step:
                pz = zo if step > 1 else z
                pc = o if step % 2 else c
                to = 2 * lax.rem(pz, 2) + pc
                send(gqo.at[4 * e + to], gqi.at[4 * e + mem], gq_s, gq_r, {"y": py, "z": pz, "c": pc})
    gqi[mem] = gqo[mem]
    scale = jnp.broadcast_to(inv_total, (8, ny * rows)).T[:, 0:1]
    q_div = (q_all.astype(F32) * scale).astype(BF16)
    g_div = (g_all.astype(F32) * scale).astype(BF16)
    order = [d for d in (2, 1, 3, 0) if d < nx]

    def pass_on(d):
        wait_bytes(pr.at[d], ps_r.at[d])
        mine = gkv[c, d] + pr[d].astype(F32)
        mine = mine.reshape(nz // 2, 2, 2 * rs, HEAD)
        px = lax.rem(x + nx - d, nx)
        for h in range(2):
            if d == 0:
                xown[h] = mine[:, h]
            xs[d, h] = mine[:, h].astype(BF16)
        sends.append(send(xs.at[d, 1 - hz], xr.at[d, 1], x_s.at[d, 1], x_r.at[d, 1], {"x": px, "z": zo}))
        if d:
            sends.append(send(xs.at[d, hz], xr.at[d, 0], x_s.at[d, 0], x_r.at[d, 0], {"x": px}))

    for i, d in enumerate(order):
        for h in range(2):
            at = pl.ds(h * half, half)
            dsv = (est[d, h] * (pgt[d, h] - delta)).astype(BF16)
            gkv[0, d, at, :] = dot(dsv, q_div, NN) * INV_ROOT
            gkv[1, d, at, :] = dot(e_b[d, h], g_div, NN)
        ps[d] = gkv[o, d].astype(BF16)
        sends.append(send(ps.at[d], pr.at[d], ps_s.at[d], ps_r.at[d], {"c": o}))
        if i >= 2:
            pass_on(order[i - 2])
    for d in order[-2:] if nx > 1 else order:
        pass_on(d)
    wait_bytes(wq4.at[0], wq_r.at[0])
    mem_z = 2 * lax.rem(zo, 2) + c
    sends.append(send(wq4.at[mem_z], wq4.at[mem_z], wq_s.at[2], wq_r.at[2], {"c": o}))
    wait_bytes(gqi.at[pl.ds(0, 4 * ny - 1)], gq_r)
    wait_bytes(wq4.at[0], wq_r.at[1])
    wait_bytes(wq4.at[0], wq_r.at[2])
    up = None
    for k in range(4):
        one = gqi[k].astype(F32)
        for e in range(1, ny):
            one = one + gqi[4 * e + k].astype(F32)
        one = dot(one.astype(BF16), wq4[k], NT)
        up = one if up is None else up + one
    pmat[...] = up
    pieces = quarter // rt
    for k in range(pieces):
        ts[k] = pmat[pl.ds(rt * k, rt), :].astype(BF16)
    pl.semaphore_wait(up_4, len(beside(4)))
    pair = lax.div(z, 2)
    per = pieces // 2
    for k in range(pieces):
        pz, pc = per * mem + k // 2, k % 2
        mine = jnp.logical_and(pz == z, pc == c)

        @pl.when(jnp.logical_not(mine))
        def _():
            send(ts.at[k], tr.at[pair], t_s, t_r, {"z": pz, "c": pc})

        @pl.when(mine)
        def _():
            tr[pair] = ts[k]

    far = sorted(range(1, nz), key=lambda k: -min(k, nz - k))

    ksum = xown[hz]
    for d in range(nx):
        for h in range(2):
            if d or h:
                wait_bytes(xr.at[d, h], x_r.at[d, h])
                ksum = ksum + xr[d, h].astype(F32)
    for k in range(nz // 2):
        for cc in range(2):
            zk[2 * k + cc] = ksum[k, rs * cc:rs * cc + rs, :].astype(BF16)
    slot = 2 * lax.div(z, 2) + c
    for dz in sorted(range(0, nz, 2), key=lambda k: -min(k, nz - k)):
        pz = lax.rem(z + dz, nz)
        for cc in (c, o):
            if dz or cc is o:
                send(zk.at[2 * lax.div(pz, 2) + cc], zr.at[slot], zk_s, zk_r, {"z": pz, "c": cc})
    zr[slot] = zk[slot]

    for e in range(1, ny):
        wait_bytes(yr.at[e], y_r.at[e])
    av = aw[pl.ds(HEAD, HEAD), pl.ds(0, rows)]
    for e in range(1, ny):
        av = av + yr[e].astype(F32)
    go = dot((av * tots[0]).astype(BF16), cotb[...], NN)
    wc = width // ns
    for k in range(ns):
        gos[k] = go[:, k * wc:(k + 1) * wc].astype(BF16)
    for dy in (2, 1, 3, 0):
        for dx in (2, 1, 3, 0):
            if dy < ny and dx < nx and (dy or dx):
                py, px = lax.rem(y + dy, ny), lax.rem(x + dx, nx)
                send(gos.at[py * nx + px], gor.at[s_me], go_s, go_r, {"y": py, "x": px})
    gor[s_me] = gos[s_me]

    l_swin.wait()
    row_at = lax.broadcasted_iota(jnp.int32, (rs, win), 0) + (rs * t_me - w0)
    pick = (lax.broadcasted_iota(jnp.int32, (rs, win), 1) == row_at).astype(F32).astype(BF16)
    sw = dot(pick, swin[...], NN)
    l_twin.wait()
    own_piece = mem == lax.div(z, per)

    @pl.when(own_piece)
    def _():
        wait_bytes(tr.at[pl.ds(0, nz // 2 - 1)], t_r)
        wait_bytes(ts.at[pl.ds(0, pieces - 1)], t_s)

    @pl.when(jnp.logical_not(own_piece))
    def _():
        wait_bytes(tr, t_r)
        wait_bytes(ts, t_s)

    up = jnp.sum(tr[...].astype(F32), axis=0)
    tw = twin[...].astype(F32)
    tw = jnp.where(c == 0, tw[0:rt, :], tw[rt:2 * rt, :])
    gt_o[...] = norm_back(tw, tgb[...], up)

    wait_bytes(gor.at[pl.ds(0, ns - 1)], go_r)
    go_o[...] = jnp.sum(gor[...].astype(F32), axis=0).astype(BF16)

    wait_bytes(zr.at[pl.ds(0, nz - 1)], zk_r)
    both = [zr[0].astype(F32), zr[1].astype(F32)]
    for k in range(2, nz):
        both[k % 2] = both[k % 2] + zr[k].astype(F32)
    both = jnp.concatenate(both, axis=1).astype(BF16)
    gs_o[...] = norm_back(sw, sgb[...], dot(both, wkv[...], NT))

    for d in sends:
        d.wait_send()
    wait_bytes(gos.at[pl.ds(0, ns - 1)], go_s)
    wait_bytes(gqo.at[pl.ds(0, 4 * ny - 1)], gq_s)
    wait_bytes(zk.at[pl.ds(0, nz - 1)], zk_s)


def write_out(a, b, c, a_o, b_o, c_o, sems):
    copies = [pltpu.make_async_copy(i, j, sems.at[k]) for k, (i, j) in enumerate(((a, a_o), (b, b_o), (c, c_o)))]
    for one in copies:
        one.start()
    for one in copies:
        one.wait()


def on_device(shape, target, source, cotangent, target_gain, source_gain, w_query, w_key, w_value, w_out):
    ny, nx, nz = shape
    rows, width = target.shape
    srows = source.shape[0]
    half = srows // 2
    rt, rs = rows // (2 * nz), srows // (2 * nz)
    win = rs if rs % 8 == 0 else rs + 4
    ns = ny * nx
    wide = ny * rows
    vm = pltpu.VMEM
    sem = pltpu.SemaphoreType.DMA
    scratch = [
        vm((half, width), BF16), vm((win, width), BF16), vm((half, width), BF16),
        vm((rows, width), BF16), vm((2 * rt, width), BF16), vm((rows, width), BF16),
        vm((rows, width), BF16), vm((1, width), F32), vm((1, width), F32),
        vm((width, 2 * HEAD), BF16), vm((HEAD, width), BF16),
        vm((nx, 2, half, 2 * HEAD), BF16), vm((ny, rows, 2 * HEAD), BF16),
        vm((nx, 2, half, wide), F32), vm((nx, 2, half, wide), F32),
        vm((nx, 2, half, wide), BF16), vm((nx, 2, half, wide), BF16),
        vm((ny, ny, 2, rows), F32), vm((2 * HEAD, wide), F32), vm((HEAD, wide), F32),
        vm((ny, HEAD, rows), BF16), vm((ny, HEAD, rows), BF16),
        vm((2, nx, srows, HEAD), F32), vm((nx, srows, HEAD), BF16), vm((nx, srows, HEAD), BF16),
        vm((nx, 2, nz // 2, 2 * rs, HEAD), BF16), vm((nx, 2, nz // 2, 2 * rs, HEAD), BF16),
        vm((2, nz // 2, 2 * rs, HEAD), F32), vm((nz, rs, HEAD), BF16), vm((nz, rs, HEAD), BF16),
        vm((4, width, HEAD), BF16), vm((4 * ny, rows // 4, HEAD), BF16), vm((4 * ny, rows // 4, HEAD), BF16),
        vm((rows // 4, width), F32), vm((rows // 4 // rt, rt, width), BF16), vm((nz // 2, rt, width), BF16),
        vm((ns, HEAD, width // ns), BF16), vm((ns, HEAD, width // ns), BF16),
        sem((11,)), sem((nx,)), sem((nx,)), sem((ny,)), sem((ny,)), sem((ny,)), sem((nx,)), sem((nx, 2)),
        sem, sem((3,)), sem, sem, sem,
        sem((nx,)), sem((nx,)), sem((ny,)), sem((ny,)), sem((ny,)), sem((nx,)), sem((nx, 2)),
        sem, sem((3,)), sem, sem, sem,
        pltpu.SemaphoreType.REGULAR, pltpu.SemaphoreType.REGULAR, pltpu.SemaphoreType.REGULAR,
    ]
    any_spec = pl.BlockSpec(memory_space=pltpu.HBM)
    vm_spec = pl.BlockSpec(memory_space=pltpu.VMEM)
    made = pl.pallas_call(
        functools.partial(kernel, (ny, nx, nz, 0, rt, rs, win)),
        out_shape=(
            vm((rt, width), BF16), vm((rs, width), BF16), vm((HEAD, width // ns), BF16),
        ),
        in_specs=[any_spec] * 9,
        out_specs=(vm_spec,) * 3,
        scratch_shapes=scratch,
        compiler_params=pltpu.CompilerParams(
            collective_id=0, has_side_effects=True, vmem_limit_bytes=56 * 1024 * 1024
        ),
    )(*(pltpu.with_memory_space_constraint(a, pltpu.HBM) for a in (
        target, source, cotangent, target_gain.reshape(1, width), source_gain.reshape(1, width),
        w_query, w_key, w_value, w_out,
    )))
    return pl.pallas_call(
        write_out,
        out_shape=tuple(jax.ShapeDtypeStruct(m.shape, m.dtype) for m in made),
        in_specs=[vm_spec] * 3,
        out_specs=(pl.BlockSpec(memory_space=pltpu.HBM),) * 3,
        scratch_shapes=[sem((3,))],
        compiler_params=pltpu.CompilerParams(vmem_limit_bytes=1024 * 1024),
    )(*made)


def solution(mesh, ny=4, nx=4):
    nz = mesh.shape["tp"] // 2
    split = Mesh(mesh.devices.reshape(ny, nx, nz, 2), ("y", "x", "z", "c"))
    sp, tp, every = ("y", "x"), ("z", "c"), ("y", "x", "z", "c")
    in_specs = (P(sp, None), P(sp, None), P(sp, None), P(), P(), P(None, tp), P(), P(), P(tp, None))
    out_specs = (P(every, None), P(every, None), P(tp, sp))
    return jax.shard_map(
        functools.partial(on_device, (ny, nx, nz)),
        mesh=split, in_specs=in_specs, out_specs=out_specs, check_vma=False,
    )
```

```python
import functools
import math

import jax
import jax.numpy as jnp
from jax import lax
from jax.experimental import pallas as pl
from jax.experimental.pallas import tpu as pltpu
from jax.sharding import Mesh
from jax.sharding import PartitionSpec as P

HEAD = 128
NORM_EPS = 1e-06
INV_ROOT = HEAD ** (-0.5)
LOG2E = math.log2(math.e)
F32, BF16 = jnp.float32, jnp.bfloat16
NN = (((1,), (0,)), ((), ()))
NT = (((1,), (1,)), ((), ()))
TN = (((0,), (0,)), ((), ()))
SHAPE = {"y": 4, "x": 4, "c": 2}


def dot(a, b, dims):
    return lax.dot_general(a, b, dims, preferred_element_type=F32)


def norm_rows(src, dst, gain):
    rows, step = src.shape[0], 16

    def one(k, carry):
        at = pl.ds(pl.multiple_of(k * step, step), step)
        v = src[at, :].astype(F32)
        r = lax.rsqrt(jnp.mean(v * v, axis=1, keepdims=True) + NORM_EPS)
        dst[at, :] = (v * r * gain[...]).astype(BF16)
        return carry

    lax.fori_loop(0, rows // step, one, 0, unroll=4)


def norm_back(rows, gain, upstream):
    r = lax.rsqrt(jnp.mean(rows * rows, axis=1, keepdims=True) + NORM_EPS)
    unit = rows * r
    pulled = upstream * gain
    return (r * (pulled - unit * jnp.mean(pulled * unit, axis=1, keepdims=True))).astype(BF16)


def wait_bytes(ref, sem):
    pltpu.make_async_copy(ref, ref, sem).wait()


def kernel(
    dims, tgt_h, src_h, cot_h, tg_h, sg_h, wq_h, wk_h, wv_h, wo_h,
    gt_o, gs_o, go_o,
    srcb, swin, sn, tgtb, twin, tn, cotb, tgb, sgb, wkv, wob,
    kv, qg, est, pgt, e_b, t_b, stat, aw, tk,
    ys, yr, gkv, ps, pr, xs, xr, xown, zk, zr,
    wq4, gqo, gqi, pmat, ts, tr, gos, gor,
    ld, kv_r, kvp_r, qg_r, st_r, y_r, ps_r, x_r, zk_r, wq_r, gq_r, t_r, go_r,
    kv_s, kvp_s, qg_s, st_s, y_s, ps_s, x_s, zk_s, wq_s, gq_s, t_s, go_s,
    up_1, up_2, up_4, seen_x, seen_y,
):
    ny, nx, nz, gsz, rt, rs, win = dims
    ns = ny * nx
    y, x, z, c = (lax.axis_index(a) for a in ("y", "x", "z", "c"))
    o = 1 - c
    s_me = y * nx + x
    zo = z + 1 - 2 * lax.rem(z, 2)
    zf = lax.rem(z - 1 + 2 * lax.rem(z, 2) + nz, nz)
    hz = lax.rem(z, 2)
    mem = 2 * hz + c
    zp = lax.select(c == 0, zo, zf)
    half = kv.shape[2]
    rows = tgtb.shape[0]
    width = tgtb.shape[1]

    barrier = pltpu.get_barrier_semaphore()

    def signal(sem, to):
        pl.semaphore_signal(sem, inc=1, device_id=to, device_id_type=pl.DeviceIdType.MESH)

    def beside(k):
        return [lax.rem(z + k, nz), lax.rem(z + nz - k, nz)] if 2 * k < nz else [lax.rem(z + k, nz)]

    peers = [{"c": o}]
    x_peers = [{"x": lax.rem(x + dx, nx)} for dx in range(1, nx)]
    y_peers = [{"y": lax.rem(y + dy, ny)} for dy in range(1, ny)]
    peers.extend(x_peers + y_peers)
    for pz in [zo, zf] if nz > 2 else [zo]:
        peers.extend([{"z": pz, "c": c}, {"z": pz, "c": o}])
    for peer in peers:
        signal(barrier, peer)

    def load(k, a, b):
        d = pltpu.make_async_copy(a, b, ld.at[k])
        d.start()
        return d

    t_me = 2 * z + c
    w0 = pl.multiple_of(lax.div(rs * t_me, 8) * 8, 8)
    l_tgt = load(4, tgt_h, tgtb)
    l_tg = load(5, tg_h, tgb)
    l_wq = load(6, wq_h, wq4.at[mem])
    l_cot = load(7, cot_h, cotb)
    l_wo = load(8, wo_h, wob)
    l_src = load(0, src_h.at[pl.ds(pl.multiple_of(c * half, half), half), :], srcb)
    l_sg = load(1, sg_h, sgb)
    l_wk = load(2, wk_h, wkv.at[:, pl.ds(0, HEAD)])
    l_wv = load(3, wv_h, wkv.at[:, pl.ds(HEAD, HEAD)])
    l_swin = load(9, src_h.at[pl.ds(w0, win), :], swin)
    l_twin = load(10, tgt_h.at[pl.ds(pl.multiple_of(2 * rt * z, 2 * rt), 2 * rt), :], twin)

    def send(a, b, s_sem, r_sem, to):
        d = pltpu.make_async_remote_copy(
            src_ref=a, dst_ref=b, send_sem=s_sem, recv_sem=r_sem,
            device_id=to, device_id_type=pl.DeviceIdType.MESH,
        )
        d.start()
        return d

    l_tgt.wait()
    l_tg.wait()
    norm_rows(tgtb, tn, tgb)
    l_wq.wait()
    qg[0, :, pl.ds(0, HEAD)] = dot(tn[...], wq4[mem], NN).astype(BF16)
    l_cot.wait()
    l_wo.wait()
    qg[0, :, pl.ds(HEAD, HEAD)] = dot(cotb[...], wob[...], NT).astype(BF16)
    pl.semaphore_wait(barrier, len(peers))
    sends = []
    x_order = [d for d in (2, 1, 3) if d < nx]
    y_order = [d for d in (2, 1, 3) if d < ny]
    for d in y_order:
        sends.append(send(qg.at[0], qg.at[d], qg_s.at[d], qg_r.at[d], {"y": lax.rem(y + d, ny)}))
    for peer in y_peers:
        signal(seen_y, peer)
    for peer in x_peers:
        signal(seen_x, peer)
    for pz in beside(1):
        signal(up_1, {"z": pz})
    sends.append(send(wq4.at[mem], wq4.at[mem], wq_s.at[0], wq_r.at[0], {"z": zo}))
    sends.append(send(wq4.at[mem], wq4.at[mem], wq_s.at[1], wq_r.at[1], {"c": o}))
    l_src.wait()
    l_sg.wait()
    norm_rows(srcb, sn, sgb)
    l_wk.wait()
    l_wv.wait()
    kv[0, c] = dot(sn[...], wkv[...], NN).astype(BF16)
    for d in x_order:
        sends.append(send(kv.at[0, c], kv.at[d, c], kv_s.at[d], kv_r.at[d], {"x": lax.rem(x + d, nx)}))
    sends.append(send(kv.at[0, c], kv.at[0, c], kvp_s.at[0], kvp_r.at[0], {"c": o}))
    pl.semaphore_wait(up_1, len(beside(1)))
    for pz in beside(2):
        signal(up_2, {"z": pz})

    for d in range(1, ny):
        wait_bytes(qg.at[d], qg_r.at[d])
    pl.semaphore_wait(up_2, len(beside(2)))
    for pz in beside(4):
        signal(up_4, {"z": pz})
    q_all = qg[:, :, pl.ds(0, HEAD)].reshape(ny * rows, HEAD)
    g_all = qg[:, :, pl.ds(HEAD, HEAD)].reshape(ny * rows, HEAD)
    tot = jnp.zeros((1, ny * rows), F32)
    tilt = jnp.zeros((1, ny * rows), F32)

    def unit(d, h, tot, tilt):
        key, val = kv[d, h, :, pl.ds(0, HEAD)], kv[d, h, :, pl.ds(HEAD, HEAD)]
        e = jnp.exp2(dot(key, q_all, NT) * (INV_ROOT * LOG2E))
        g = dot(val, g_all, NT)
        t = e * g
        est[d, h] = e
        pgt[d, h] = g
        e_b[d, h] = e.astype(BF16)
        t_b[d, h] = t.astype(BF16)
        return tot + jnp.sum(e, axis=0, keepdims=True), tilt + jnp.sum(t, axis=0, keepdims=True)

    def unit_sums(d, h, first):
        both = dot(kv[d, h], e_b[d, h], TN)
        one = dot(kv[d, h, :, pl.ds(0, HEAD)], t_b[d, h], TN)
        aw[...] = both if first else aw[...] + both
        tk[...] = one if first else tk[...] + one

    x_seen = [d for d in (1, 3, 2) if d < nx]
    tot, tilt = unit(0, c, tot, tilt)
    before = 0
    for d in x_seen:
        wait_bytes(kv.at[d, c], kv_r.at[d])
        sends.append(send(kv.at[d, c], kv.at[d, c], kvp_s.at[d], kvp_r.at[d], {"c": o}))
        wait_bytes(kv.at[before, o], kvp_r.at[before])
        tot, tilt = unit(before, o, tot, tilt)
        tot, tilt = unit(d, c, tot, tilt)
        before = d
    wait_bytes(kv.at[before, o], kvp_r.at[before])
    tot, tilt = unit(before, o, tot, tilt)

    for e in range(ny):
        stat[0, e, 0:1, :] = tot[:, e * rows:(e + 1) * rows]
        stat[0, e, 1:2, :] = tilt[:, e * rows:(e + 1) * rows]
    for d in y_order:
        sends.append(send(stat.at[0], stat.at[d], st_s.at[d], st_r.at[d], {"y": lax.rem(y + d, ny)}))
    for d in range(nx):
        for h in range(2):
            unit_sums(d, h, d + h == 0)
    for e in y_order:
        ys[e] = aw[pl.ds(HEAD, HEAD), pl.ds(e * rows, rows)].astype(BF16)
        sends.append(send(ys.at[e], yr.at[e], y_s.at[e], y_r.at[e], {"y": lax.rem(y + ny - e, ny)}))
    for d in range(1, ny):
        wait_bytes(stat.at[d], st_r.at[d])
    tots, deltas = [], []
    for e in range(ny):
        both = stat[0, e]
        for d in range(1, ny):
            both = both + stat[d, (e - d) % ny]
        tots.append(1.0 / both[0:1, :])
        deltas.append(both[1:2, :] / both[0:1, :])
    inv_total = jnp.concatenate(tots, axis=1)
    delta = jnp.concatenate(deltas, axis=1)

    pl.semaphore_wait(seen_y, len(y_peers))
    gq = ((tk[...] - delta * aw[pl.ds(0, HEAD), :]) * (inv_total * INV_ROOT)).T.astype(BF16)
    quarter = rows // 4
    for e in range(ny):
        for k in range(4):
            gqo[4 * e + k] = gq[e * rows + k * quarter:e * rows + (k + 1) * quarter, :]
    for e in y_order + [0]:
        py = lax.rem(y + ny - e, ny)
        for step in (2, 3, 1, 0):
            if e or step:
                pz = zo if step > 1 else z
                pc = o if step % 2 else c
                to = 2 * lax.rem(pz, 2) + pc
                send(gqo.at[4 * e + to], gqi.at[4 * e + mem], gq_s, gq_r, {"y": py, "z": pz, "c": pc})
    gqi[mem] = gqo[mem]
    pl.semaphore_wait(seen_x, len(x_peers))
    scale = jnp.broadcast_to(inv_total, (8, ny * rows)).T[:, 0:1]
    q_div = (q_all.astype(F32) * scale).astype(BF16)
    g_div = (g_all.astype(F32) * scale).astype(BF16)
    order = [d for d in (2, 1, 3, 0) if d < nx]

    def pass_on(d):
        wait_bytes(pr.at[d], ps_r.at[d])
        mine = gkv[c, d] + pr[d].astype(F32)
        mine = mine.reshape(nz // 2, 2, 2 * rs, HEAD)
        px = lax.rem(x + nx - d, nx)
        for h in range(2):
            if d == 0:
                xown[h] = mine[:, h]
            xs[d, h] = mine[:, h].astype(BF16)
        sends.append(send(xs.at[d, 1 - hz], xr.at[d, 1], x_s.at[d, 1], x_r.at[d, 1], {"x": px, "z": zp}))
        if d:
            sends.append(send(xs.at[d, hz], xr.at[d, 0], x_s.at[d, 0], x_r.at[d, 0], {"x": px}))

    for i, d in enumerate(order):
        for h in range(2):
            at = pl.ds(h * half, half)
            dsv = (est[d, h] * (pgt[d, h] - delta)).astype(BF16)
            gkv[0, d, at, :] = dot(dsv, q_div, NN) * INV_ROOT
            gkv[1, d, at, :] = dot(e_b[d, h], g_div, NN)
        ps[d] = gkv[o, d].astype(BF16)
        sends.append(send(ps.at[d], pr.at[d], ps_s.at[d], ps_r.at[d], {"c": o}))
        if i >= 2:
            pass_on(order[i - 2])
    for d in order[-2:] if nx > 1 else order:
        pass_on(d)
    wait_bytes(wq4.at[0], wq_r.at[0])
    mem_z = 2 * lax.rem(zo, 2) + c
    sends.append(send(wq4.at[mem_z], wq4.at[mem_z], wq_s.at[2], wq_r.at[2], {"c": o}))
    wait_bytes(gqi.at[pl.ds(0, 4 * ny - 1)], gq_r)
    wait_bytes(wq4.at[0], wq_r.at[1])
    wait_bytes(wq4.at[0], wq_r.at[2])
    up = None
    for k in range(4):
        one = gqi[k].astype(F32)
        for e in range(1, ny):
            one = one + gqi[4 * e + k].astype(F32)
        one = dot(one.astype(BF16), wq4[k], NT)
        up = one if up is None else up + one
    pmat[...] = up
    pieces = quarter // rt
    for k in range(pieces):
        ts[k] = pmat[pl.ds(rt * k, rt), :].astype(BF16)
    pl.semaphore_wait(up_4, len(beside(4)))
    pair = lax.div(z, 2)
    per = pieces // 2
    for k in range(pieces):
        pz, pc = per * mem + k // 2, k % 2
        mine = jnp.logical_and(pz == z, pc == c)

        @pl.when(jnp.logical_not(mine))
        def _():
            send(ts.at[k], tr.at[pair], t_s, t_r, {"z": pz, "c": pc})

        @pl.when(mine)
        def _():
            tr[pair] = ts[k]

    far = sorted(range(1, nz), key=lambda k: -min(k, nz - k))

    ksum = xown[hz]
    for d in range(nx):
        for h in range(2):
            if d or h:
                wait_bytes(xr.at[d, h], x_r.at[d, h])
                ksum = ksum + xr[d, h].astype(F32)
    for k in range(nz // 2):
        for cc in range(2):
            zk[2 * k + cc] = ksum[k, rs * cc:rs * cc + rs, :].astype(BF16)
    slot = 2 * lax.div(z, 2) + c
    for dz in sorted(range(0, nz, 2), key=lambda k: -min(k, nz - k)):
        pz = lax.rem(z + dz, nz)
        for cc in (c, o):
            if dz or cc is o:
                send(zk.at[2 * lax.div(pz, 2) + cc], zr.at[slot], zk_s, zk_r, {"z": pz, "c": cc})
    zr[slot] = zk[slot]

    for e in range(1, ny):
        wait_bytes(yr.at[e], y_r.at[e])
    av = aw[pl.ds(HEAD, HEAD), pl.ds(0, rows)]
    for e in range(1, ny):
        av = av + yr[e].astype(F32)
    go = dot((av * tots[0]).astype(BF16), cotb[...], NN)
    wc = width // ns
    for k in range(ns):
        gos[k] = go[:, k * wc:(k + 1) * wc].astype(BF16)
    for dy in (2, 1, 3, 0):
        for dx in (2, 1, 3, 0):
            if dy < ny and dx < nx and (dy or dx):
                py, px = lax.rem(y + dy, ny), lax.rem(x + dx, nx)
                send(gos.at[py * nx + px], gor.at[s_me], go_s, go_r, {"y": py, "x": px})
    gor[s_me] = gos[s_me]

    l_swin.wait()
    row_at = lax.broadcasted_iota(jnp.int32, (rs, win), 0) + (rs * t_me - w0)
    pick = (lax.broadcasted_iota(jnp.int32, (rs, win), 1) == row_at).astype(F32).astype(BF16)
    sw = dot(pick, swin[...], NN)
    l_twin.wait()
    own_piece = mem == lax.div(z, per)

    @pl.when(own_piece)
    def _():
        wait_bytes(tr.at[pl.ds(0, nz // 2 - 1)], t_r)
        wait_bytes(ts.at[pl.ds(0, pieces - 1)], t_s)

    @pl.when(jnp.logical_not(own_piece))
    def _():
        wait_bytes(tr, t_r)
        wait_bytes(ts, t_s)

    up = jnp.sum(tr[...].astype(F32), axis=0)
    tw = twin[...].astype(F32)
    tw = jnp.where(c == 0, tw[0:rt, :], tw[rt:2 * rt, :])
    gt_o[...] = norm_back(tw, tgb[...], up)

    wait_bytes(gor.at[pl.ds(0, ns - 1)], go_r)
    go_o[...] = jnp.sum(gor[...].astype(F32), axis=0).astype(BF16)

    wait_bytes(zr.at[pl.ds(0, nz - 1)], zk_r)
    both = [zr[0].astype(F32), zr[1].astype(F32)]
    for k in range(2, nz):
        both[k % 2] = both[k % 2] + zr[k].astype(F32)
    both = jnp.concatenate(both, axis=1).astype(BF16)
    gs_o[...] = norm_back(sw, sgb[...], dot(both, wkv[...], NT))

    for d in sends:
        d.wait_send()
    wait_bytes(gos.at[pl.ds(0, ns - 1)], go_s)
    wait_bytes(gqo.at[pl.ds(0, 4 * ny - 1)], gq_s)
    wait_bytes(zk.at[pl.ds(0, nz - 1)], zk_s)


def write_out(a, b, c, a_o, b_o, c_o, sems):
    copies = [pltpu.make_async_copy(i, j, sems.at[k]) for k, (i, j) in enumerate(((a, a_o), (b, b_o), (c, c_o)))]
    for one in copies:
        one.start()
    for one in copies:
        one.wait()


def on_device(shape, target, source, cotangent, target_gain, source_gain, w_query, w_key, w_value, w_out):
    ny, nx, nz = shape
    rows, width = target.shape
    srows = source.shape[0]
    half = srows // 2
    rt, rs = rows // (2 * nz), srows // (2 * nz)
    win = rs if rs % 8 == 0 else rs + 4
    ns = ny * nx
    wide = ny * rows
    vm = pltpu.VMEM
    sem = pltpu.SemaphoreType.DMA
    scratch = [
        vm((half, width), BF16), vm((win, width), BF16), vm((half, width), BF16),
        vm((rows, width), BF16), vm((2 * rt, width), BF16), vm((rows, width), BF16),
        vm((rows, width), BF16), vm((1, width), F32), vm((1, width), F32),
        vm((width, 2 * HEAD), BF16), vm((HEAD, width), BF16),
        vm((nx, 2, half, 2 * HEAD), BF16), vm((ny, rows, 2 * HEAD), BF16),
        vm((nx, 2, half, wide), F32), vm((nx, 2, half, wide), F32),
        vm((nx, 2, half, wide), BF16), vm((nx, 2, half, wide), BF16),
        vm((ny, ny, 2, rows), F32), vm((2 * HEAD, wide), F32), vm((HEAD, wide), F32),
        vm((ny, HEAD, rows), BF16), vm((ny, HEAD, rows), BF16),
        vm((2, nx, srows, HEAD), F32), vm((nx, srows, HEAD), BF16), vm((nx, srows, HEAD), BF16),
        vm((nx, 2, nz // 2, 2 * rs, HEAD), BF16), vm((nx, 2, nz // 2, 2 * rs, HEAD), BF16),
        vm((2, nz // 2, 2 * rs, HEAD), F32), vm((nz, rs, HEAD), BF16), vm((nz, rs, HEAD), BF16),
        vm((4, width, HEAD), BF16), vm((4 * ny, rows // 4, HEAD), BF16), vm((4 * ny, rows // 4, HEAD), BF16),
        vm((rows // 4, width), F32), vm((rows // 4 // rt, rt, width), BF16), vm((nz // 2, rt, width), BF16),
        vm((ns, HEAD, width // ns), BF16), vm((ns, HEAD, width // ns), BF16),
        sem((11,)), sem((nx,)), sem((nx,)), sem((ny,)), sem((ny,)), sem((ny,)), sem((nx,)), sem((nx, 2)),
        sem, sem((3,)), sem, sem, sem,
        sem((nx,)), sem((nx,)), sem((ny,)), sem((ny,)), sem((ny,)), sem((nx,)), sem((nx, 2)),
        sem, sem((3,)), sem, sem, sem,
        pltpu.SemaphoreType.REGULAR, pltpu.SemaphoreType.REGULAR, pltpu.SemaphoreType.REGULAR,
        pltpu.SemaphoreType.REGULAR, pltpu.SemaphoreType.REGULAR,
    ]
    any_spec = pl.BlockSpec(memory_space=pltpu.HBM)
    vm_spec = pl.BlockSpec(memory_space=pltpu.VMEM)
    made = pl.pallas_call(
        functools.partial(kernel, (ny, nx, nz, 0, rt, rs, win)),
        out_shape=(
            vm((rt, width), BF16), vm((rs, width), BF16), vm((HEAD, width // ns), BF16),
        ),
        in_specs=[any_spec] * 9,
        out_specs=(vm_spec,) * 3,
        scratch_shapes=scratch,
        compiler_params=pltpu.CompilerParams(
            collective_id=0, has_side_effects=True, vmem_limit_bytes=56 * 1024 * 1024
        ),
    )(*(pltpu.with_memory_space_constraint(a, pltpu.HBM) for a in (
        target, source, cotangent, target_gain.reshape(1, width), source_gain.reshape(1, width),
        w_query, w_key, w_value, w_out,
    )))
    return pl.pallas_call(
        write_out,
        out_shape=tuple(jax.ShapeDtypeStruct(m.shape, m.dtype) for m in made),
        in_specs=[vm_spec] * 3,
        out_specs=(pl.BlockSpec(memory_space=pltpu.HBM),) * 3,
        scratch_shapes=[sem((3,))],
        compiler_params=pltpu.CompilerParams(vmem_limit_bytes=1024 * 1024),
    )(*made)


def solution(mesh, ny=4, nx=4):
    nz = mesh.shape["tp"] // 2
    split = Mesh(mesh.devices.reshape(ny, nx, nz, 2), ("y", "x", "z", "c"))
    sp, tp, every = ("y", "x"), ("z", "c"), ("y", "x", "z", "c")
    in_specs = (P(sp, None), P(sp, None), P(sp, None), P(), P(), P(None, tp), P(), P(), P(tp, None))
    out_specs = (P(every, None), P(every, None), P(tp, sp))
    return jax.shard_map(
        functools.partial(on_device, (ny, nx, nz)),
        mesh=split, in_specs=in_specs, out_specs=out_specs, check_vma=False,
    )
```

```python
import functools
import math

import jax
import jax.numpy as jnp
from jax import lax
from jax.experimental import pallas as pl
from jax.experimental.pallas import tpu as pltpu
from jax.sharding import Mesh
from jax.sharding import PartitionSpec as P

HEAD = 128
NORM_EPS = 1e-06
INV_ROOT = HEAD ** (-0.5)
LOG2E = math.log2(math.e)
F32, BF16 = jnp.float32, jnp.bfloat16
NN = (((1,), (0,)), ((), ()))
NT = (((1,), (1,)), ((), ()))
TN = (((0,), (0,)), ((), ()))
SHAPE = {"y": 4, "x": 4, "c": 2}


def dot(a, b, dims):
    return lax.dot_general(a, b, dims, preferred_element_type=F32)


def norm_rows(src, dst, gain):
    rows, step = src.shape[0], 16

    def one(k, carry):
        at = pl.ds(pl.multiple_of(k * step, step), step)
        v = src[at, :].astype(F32)
        r = lax.rsqrt(jnp.mean(v * v, axis=1, keepdims=True) + NORM_EPS)
        dst[at, :] = (v * r * gain[...]).astype(BF16)
        return carry

    lax.fori_loop(0, rows // step, one, 0, unroll=4)


def norm_back(rows, gain, upstream):
    r = lax.rsqrt(jnp.mean(rows * rows, axis=1, keepdims=True) + NORM_EPS)
    unit = rows * r
    pulled = upstream * gain
    return (r * (pulled - unit * jnp.mean(pulled * unit, axis=1, keepdims=True))).astype(BF16)


def wait_bytes(ref, sem):
    pltpu.make_async_copy(ref, ref, sem).wait()


def kernel(
    dims, tgt_h, src_h, cot_h, tg_h, sg_h, wq_h, wk_h, wv_h, wo_h,
    gt_o, gs_o, go_o,
    srcb, swin, sn, tgtb, twin, tn, cotb, tgb, sgb, wkv, wob,
    kv, qg, est, pgt, lhs, t_b, rhs, stat, aw, tk,
    ys, yr, gkv, ps, pr, xs, xr, xown, zk, zr,
    wq4, gqo, gqi, pmat, ts, tr, gos, gor,
    ld, kv_r, kvp_r, qg_r, st_r, y_r, ps_r, x_r, zk_r, wq_r, gq_r, t_r, go_r,
    kv_s, kvp_s, qg_s, st_s, y_s, ps_s, x_s, zk_s, wq_s, gq_s, t_s, go_s,
    up_1, up_2, up_4, seen_x, seen_y,
):
    ny, nx, nz, gsz, rt, rs, win = dims
    ns = ny * nx
    y, x, z, c = (lax.axis_index(a) for a in ("y", "x", "z", "c"))
    o = 1 - c
    s_me = y * nx + x
    zo = z + 1 - 2 * lax.rem(z, 2)
    zf = lax.rem(z - 1 + 2 * lax.rem(z, 2) + nz, nz)
    hz = lax.rem(z, 2)
    mem = 2 * hz + c
    zp = lax.select(c == 0, zo, zf)
    half = kv.shape[2]
    rows = tgtb.shape[0]
    width = tgtb.shape[1]

    barrier = pltpu.get_barrier_semaphore()

    def signal(sem, to):
        pl.semaphore_signal(sem, inc=1, device_id=to, device_id_type=pl.DeviceIdType.MESH)

    def beside(k):
        return [lax.rem(z + k, nz), lax.rem(z + nz - k, nz)] if 2 * k < nz else [lax.rem(z + k, nz)]

    peers = [{"c": o}]
    x_peers = [{"x": lax.rem(x + dx, nx)} for dx in range(1, nx)]
    y_peers = [{"y": lax.rem(y + dy, ny)} for dy in range(1, ny)]
    peers.extend(x_peers + y_peers)
    for pz in [zo, zf] if nz > 2 else [zo]:
        peers.extend([{"z": pz, "c": c}, {"z": pz, "c": o}])
    for peer in peers:
        signal(barrier, peer)

    def load(k, a, b):
        d = pltpu.make_async_copy(a, b, ld.at[k])
        d.start()
        return d

    t_me = 2 * z + c
    w0 = pl.multiple_of(lax.div(rs * t_me, 8) * 8, 8)
    l_tgt = load(4, tgt_h, tgtb)
    l_tg = load(5, tg_h, tgb)
    l_wq = load(6, wq_h, wq4.at[mem])
    l_cot = load(7, cot_h, cotb)
    l_wo = load(8, wo_h, wob)
    l_src = load(0, src_h.at[pl.ds(pl.multiple_of(c * half, half), half), :], srcb)
    l_sg = load(1, sg_h, sgb)
    l_wk = load(2, wk_h, wkv.at[:, pl.ds(0, HEAD)])
    l_wv = load(3, wv_h, wkv.at[:, pl.ds(HEAD, HEAD)])
    l_swin = load(9, src_h.at[pl.ds(w0, win), :], swin)
    l_twin = load(10, tgt_h.at[pl.ds(pl.multiple_of(2 * rt * z, 2 * rt), 2 * rt), :], twin)

    def send(a, b, s_sem, r_sem, to):
        d = pltpu.make_async_remote_copy(
            src_ref=a, dst_ref=b, send_sem=s_sem, recv_sem=r_sem,
            device_id=to, device_id_type=pl.DeviceIdType.MESH,
        )
        d.start()
        return d

    l_tgt.wait()
    l_tg.wait()
    norm_rows(tgtb, tn, tgb)
    l_wq.wait()
    qg[0, :, pl.ds(0, HEAD)] = dot(tn[...], wq4[mem], NN).astype(BF16)
    l_cot.wait()
    l_wo.wait()
    qg[0, :, pl.ds(HEAD, HEAD)] = dot(cotb[...], wob[...], NT).astype(BF16)
    pl.semaphore_wait(barrier, len(peers))
    sends = []
    x_order = [d for d in (1, 3, 2) if d < nx]
    y_order = [d for d in (2, 1, 3) if d < ny]
    for d in y_order:
        sends.append(send(qg.at[0], qg.at[d], qg_s.at[d], qg_r.at[d], {"y": lax.rem(y + d, ny)}))
    for peer in y_peers:
        signal(seen_y, peer)
    for peer in x_peers:
        signal(seen_x, peer)
    for pz in beside(1):
        signal(up_1, {"z": pz})
    sends.append(send(wq4.at[mem], wq4.at[mem], wq_s.at[0], wq_r.at[0], {"z": zo}))
    sends.append(send(wq4.at[mem], wq4.at[mem], wq_s.at[1], wq_r.at[1], {"c": o}))
    l_src.wait()
    l_sg.wait()
    norm_rows(srcb, sn, sgb)
    l_wk.wait()
    l_wv.wait()
    kv[0, c] = dot(sn[...], wkv[...], NN).astype(BF16)
    for d in x_order:
        sends.append(send(kv.at[0, c], kv.at[d, c], kv_s.at[d], kv_r.at[d], {"x": lax.rem(x + d, nx)}))
    sends.append(send(kv.at[0, c], kv.at[0, c], kvp_s.at[0], kvp_r.at[0], {"c": o}))
    pl.semaphore_wait(up_1, len(beside(1)))
    for pz in beside(2):
        signal(up_2, {"z": pz})

    for d in range(1, ny):
        wait_bytes(qg.at[d], qg_r.at[d])
    pl.semaphore_wait(up_2, len(beside(2)))
    for pz in beside(4):
        signal(up_4, {"z": pz})
    q_all = qg[:, :, pl.ds(0, HEAD)].reshape(ny * rows, HEAD)
    g_all = qg[:, :, pl.ds(HEAD, HEAD)].reshape(ny * rows, HEAD)
    tot = jnp.zeros((1, ny * rows), F32)
    tilt = jnp.zeros((1, ny * rows), F32)

    def unit(d, h, tot, tilt):
        key, val = kv[d, h, :, pl.ds(0, HEAD)], kv[d, h, :, pl.ds(HEAD, HEAD)]
        e = jnp.exp2(dot(key, q_all, NT) * (INV_ROOT * LOG2E))
        g = dot(val, g_all, NT)
        t = e * g
        est[d, h] = e
        pgt[d, h] = g
        lhs[1, d, h] = e.astype(BF16)
        t_b[d, h] = t.astype(BF16)
        return tot + jnp.sum(e, axis=0, keepdims=True), tilt + jnp.sum(t, axis=0, keepdims=True)

    def unit_sums(d, h, first):
        both = dot(kv[d, h], lhs[1, d, h], TN)
        one = dot(kv[d, h, :, pl.ds(0, HEAD)], t_b[d, h], TN)
        aw[...] = both if first else aw[...] + both
        tk[...] = one if first else tk[...] + one

    x_seen = [d for d in (1, 3, 2) if d < nx]
    tot, tilt = unit(0, c, tot, tilt)
    before = 0
    for d in x_seen:
        wait_bytes(kv.at[d, c], kv_r.at[d])
        sends.append(send(kv.at[d, c], kv.at[d, c], kvp_s.at[d], kvp_r.at[d], {"c": o}))
        wait_bytes(kv.at[before, o], kvp_r.at[before])
        tot, tilt = unit(before, o, tot, tilt)
        tot, tilt = unit(d, c, tot, tilt)
        before = d
    wait_bytes(kv.at[before, o], kvp_r.at[before])
    tot, tilt = unit(before, o, tot, tilt)

    for e in range(ny):
        stat[0, e, 0:1, :] = tot[:, e * rows:(e + 1) * rows]
        stat[0, e, 1:2, :] = tilt[:, e * rows:(e + 1) * rows]
    for d in y_order:
        sends.append(send(stat.at[0], stat.at[d], st_s.at[d], st_r.at[d], {"y": lax.rem(y + d, ny)}))
    for d in range(nx):
        for h in range(2):
            unit_sums(d, h, d + h == 0)
    for e in y_order:
        ys[e] = aw[pl.ds(HEAD, HEAD), pl.ds(e * rows, rows)].astype(BF16)
        sends.append(send(ys.at[e], yr.at[e], y_s.at[e], y_r.at[e], {"y": lax.rem(y + ny - e, ny)}))
    for d in range(1, ny):
        wait_bytes(stat.at[d], st_r.at[d])
    tots, deltas = [], []
    for e in range(ny):
        both = stat[0, e]
        for d in range(1, ny):
            both = both + stat[d, (e - d) % ny]
        tots.append(1.0 / both[0:1, :])
        deltas.append(both[1:2, :] / both[0:1, :])
    inv_total = jnp.concatenate(tots, axis=1)
    delta = jnp.concatenate(deltas, axis=1)

    pl.semaphore_wait(seen_y, len(y_peers))
    gq = ((tk[...] - delta * aw[pl.ds(0, HEAD), :]) * (inv_total * INV_ROOT)).T.astype(BF16)
    quarter = rows // 4
    for e in range(ny):
        for k in range(4):
            gqo[4 * e + k] = gq[e * rows + k * quarter:e * rows + (k + 1) * quarter, :]
    for e in y_order + [0]:
        py = lax.rem(y + ny - e, ny)
        for step in (2, 3, 1, 0):
            if e or step:
                pz = zo if step > 1 else z
                pc = o if step % 2 else c
                to = 2 * lax.rem(pz, 2) + pc
                send(gqo.at[4 * e + to], gqi.at[4 * e + mem], gq_s, gq_r, {"y": py, "z": pz, "c": pc})
    gqi[mem] = gqo[mem]
    pl.semaphore_wait(seen_x, len(x_peers))
    scale = jnp.broadcast_to(inv_total, (8, ny * rows)).T[:, 0:1]
    rhs[0] = (q_all.astype(F32) * (scale * INV_ROOT)).astype(BF16)
    rhs[1] = (g_all.astype(F32) * scale).astype(BF16)
    order = [d for d in (2, 1, 3, 0) if d < nx]

    def other(d):
        for h in range(2):
            lhs[0, d, h] = (est[d, h] * (pgt[d, h] - delta)).astype(BF16)
            ps[d, pl.ds(h * half, half), :] = dot(lhs[o, d, h], rhs[o], NN).astype(BF16)
        sends.append(send(ps.at[d], pr.at[d], ps_s.at[d], ps_r.at[d], {"c": o}))

    def own(d):
        for h in range(2):
            gkv[d, pl.ds(h * half, half), :] = dot(lhs[c, d, h], rhs[c], NN)

    def pass_on(d):
        wait_bytes(pr.at[d], ps_r.at[d])
        mine = gkv[d] + pr[d].astype(F32)
        mine = mine.reshape(nz // 2, 2, 2 * rs, HEAD)
        px = lax.rem(x + nx - d, nx)
        for h in range(2):
            if d == 0:
                xown[h] = mine[:, h]
            xs[d, h] = mine[:, h].astype(BF16)
        sends.append(send(xs.at[d, 1 - hz], xr.at[d, 1], x_s.at[d, 1], x_r.at[d, 1], {"x": px, "z": zp}))
        if d:
            sends.append(send(xs.at[d, hz], xr.at[d, 0], x_s.at[d, 0], x_r.at[d, 0], {"x": px}))

    steps = [(other, order[0])]
    for i in range(len(order)):
        if i + 1 < len(order):
            steps.append((other, order[i + 1]))
        steps.append((own, order[i]))
        if i:
            steps.append((pass_on, order[i - 1]))
    for step, d in steps:
        step(d)
    wait_bytes(wq4.at[0], wq_r.at[0])
    mem_z = 2 * lax.rem(zo, 2) + c
    sends.append(send(wq4.at[mem_z], wq4.at[mem_z], wq_s.at[2], wq_r.at[2], {"c": o}))
    pass_on(order[-1])
    wait_bytes(gqi.at[pl.ds(0, 4 * ny - 1)], gq_r)
    wait_bytes(wq4.at[0], wq_r.at[1])
    wait_bytes(wq4.at[0], wq_r.at[2])
    up = None
    for k in range(4):
        one = gqi[k].astype(F32)
        for e in range(1, ny):
            one = one + gqi[4 * e + k].astype(F32)
        one = dot(one.astype(BF16), wq4[k], NT)
        up = one if up is None else up + one
    pmat[...] = up
    pieces = quarter // rt
    for k in range(pieces):
        ts[k] = pmat[pl.ds(rt * k, rt), :].astype(BF16)
    pl.semaphore_wait(up_4, len(beside(4)))
    pair = lax.div(z, 2)
    per = pieces // 2
    for k in range(pieces):
        pz, pc = per * mem + k // 2, k % 2
        mine = jnp.logical_and(pz == z, pc == c)

        @pl.when(jnp.logical_not(mine))
        def _():
            send(ts.at[k], tr.at[pair], t_s, t_r, {"z": pz, "c": pc})

        @pl.when(mine)
        def _():
            tr[pair] = ts[k]

    far = sorted(range(1, nz), key=lambda k: -min(k, nz - k))

    ksum = xown[hz]
    for d in range(nx):
        for h in range(2):
            if d or h:
                wait_bytes(xr.at[d, h], x_r.at[d, h])
                ksum = ksum + xr[d, h].astype(F32)
    for k in range(nz // 2):
        for cc in range(2):
            zk[2 * k + cc] = ksum[k, rs * cc:rs * cc + rs, :].astype(BF16)
    slot = 2 * lax.div(z, 2) + c
    for dz in sorted(range(0, nz, 2), key=lambda k: -min(k, nz - k)):
        pz = lax.rem(z + dz, nz)
        for cc in (c, o):
            if dz or cc is o:
                send(zk.at[2 * lax.div(pz, 2) + cc], zr.at[slot], zk_s, zk_r, {"z": pz, "c": cc})
    zr[slot] = zk[slot]

    for e in range(1, ny):
        wait_bytes(yr.at[e], y_r.at[e])
    av = aw[pl.ds(HEAD, HEAD), pl.ds(0, rows)]
    for e in range(1, ny):
        av = av + yr[e].astype(F32)
    go = dot((av * tots[0]).astype(BF16), cotb[...], NN)
    wc = width // ns
    for k in range(ns):
        gos[k] = go[:, k * wc:(k + 1) * wc].astype(BF16)
    for dy in (2, 1, 3, 0):
        for dx in (2, 1, 3, 0):
            if dy < ny and dx < nx and (dy or dx):
                py, px = lax.rem(y + dy, ny), lax.rem(x + dx, nx)
                send(gos.at[py * nx + px], gor.at[s_me], go_s, go_r, {"y": py, "x": px})
    gor[s_me] = gos[s_me]

    l_swin.wait()
    row_at = lax.broadcasted_iota(jnp.int32, (rs, win), 0) + (rs * t_me - w0)
    pick = (lax.broadcasted_iota(jnp.int32, (rs, win), 1) == row_at).astype(F32).astype(BF16)
    sw = dot(pick, swin[...], NN)
    l_twin.wait()
    own_piece = mem == lax.div(z, per)

    @pl.when(own_piece)
    def _():
        wait_bytes(tr.at[pl.ds(0, nz // 2 - 1)], t_r)
        wait_bytes(ts.at[pl.ds(0, pieces - 1)], t_s)

    @pl.when(jnp.logical_not(own_piece))
    def _():
        wait_bytes(tr, t_r)
        wait_bytes(ts, t_s)

    up = jnp.sum(tr[...].astype(F32), axis=0)
    tw = twin[...].astype(F32)
    tw = jnp.where(c == 0, tw[0:rt, :], tw[rt:2 * rt, :])
    gt_o[...] = norm_back(tw, tgb[...], up)

    wait_bytes(gor.at[pl.ds(0, ns - 1)], go_r)
    go_o[...] = jnp.sum(gor[...].astype(F32), axis=0).astype(BF16)

    wait_bytes(zr.at[pl.ds(0, nz - 1)], zk_r)
    both = [zr[0].astype(F32), zr[1].astype(F32)]
    for k in range(2, nz):
        both[k % 2] = both[k % 2] + zr[k].astype(F32)
    both = jnp.concatenate(both, axis=1).astype(BF16)
    gs_o[...] = norm_back(sw, sgb[...], dot(both, wkv[...], NT))

    for d in sends:
        d.wait_send()
    wait_bytes(gos.at[pl.ds(0, ns - 1)], go_s)
    wait_bytes(gqo.at[pl.ds(0, 4 * ny - 1)], gq_s)
    wait_bytes(zk.at[pl.ds(0, nz - 1)], zk_s)


def write_out(a, b, c, a_o, b_o, c_o, sems):
    copies = [pltpu.make_async_copy(i, j, sems.at[k]) for k, (i, j) in enumerate(((a, a_o), (b, b_o), (c, c_o)))]
    for one in copies:
        one.start()
    for one in copies:
        one.wait()


def on_device(shape, target, source, cotangent, target_gain, source_gain, w_query, w_key, w_value, w_out):
    ny, nx, nz = shape
    rows, width = target.shape
    srows = source.shape[0]
    half = srows // 2
    rt, rs = rows // (2 * nz), srows // (2 * nz)
    win = rs if rs % 8 == 0 else rs + 4
    ns = ny * nx
    wide = ny * rows
    vm = pltpu.VMEM
    sem = pltpu.SemaphoreType.DMA
    scratch = [
        vm((half, width), BF16), vm((win, width), BF16), vm((half, width), BF16),
        vm((rows, width), BF16), vm((2 * rt, width), BF16), vm((rows, width), BF16),
        vm((rows, width), BF16), vm((1, width), F32), vm((1, width), F32),
        vm((width, 2 * HEAD), BF16), vm((HEAD, width), BF16),
        vm((nx, 2, half, 2 * HEAD), BF16), vm((ny, rows, 2 * HEAD), BF16),
        vm((nx, 2, half, wide), F32), vm((nx, 2, half, wide), F32),
        vm((2, nx, 2, half, wide), BF16), vm((nx, 2, half, wide), BF16), vm((2, wide, HEAD), BF16),
        vm((ny, ny, 2, rows), F32), vm((2 * HEAD, wide), F32), vm((HEAD, wide), F32),
        vm((ny, HEAD, rows), BF16), vm((ny, HEAD, rows), BF16),
        vm((nx, srows, HEAD), F32), vm((nx, srows, HEAD), BF16), vm((nx, srows, HEAD), BF16),
        vm((nx, 2, nz // 2, 2 * rs, HEAD), BF16), vm((nx, 2, nz // 2, 2 * rs, HEAD), BF16),
        vm((2, nz // 2, 2 * rs, HEAD), F32), vm((nz, rs, HEAD), BF16), vm((nz, rs, HEAD), BF16),
        vm((4, width, HEAD), BF16), vm((4 * ny, rows // 4, HEAD), BF16), vm((4 * ny, rows // 4, HEAD), BF16),
        vm((rows // 4, width), F32), vm((rows // 4 // rt, rt, width), BF16), vm((nz // 2, rt, width), BF16),
        vm((ns, HEAD, width // ns), BF16), vm((ns, HEAD, width // ns), BF16),
        sem((11,)), sem((nx,)), sem((nx,)), sem((ny,)), sem((ny,)), sem((ny,)), sem((nx,)), sem((nx, 2)),
        sem, sem((3,)), sem, sem, sem,
        sem((nx,)), sem((nx,)), sem((ny,)), sem((ny,)), sem((ny,)), sem((nx,)), sem((nx, 2)),
        sem, sem((3,)), sem, sem, sem,
        pltpu.SemaphoreType.REGULAR, pltpu.SemaphoreType.REGULAR, pltpu.SemaphoreType.REGULAR,
        pltpu.SemaphoreType.REGULAR, pltpu.SemaphoreType.REGULAR,
    ]
    any_spec = pl.BlockSpec(memory_space=pltpu.HBM)
    vm_spec = pl.BlockSpec(memory_space=pltpu.VMEM)
    made = pl.pallas_call(
        functools.partial(kernel, (ny, nx, nz, 0, rt, rs, win)),
        out_shape=(
            vm((rt, width), BF16), vm((rs, width), BF16), vm((HEAD, width // ns), BF16),
        ),
        in_specs=[any_spec] * 9,
        out_specs=(vm_spec,) * 3,
        scratch_shapes=scratch,
        compiler_params=pltpu.CompilerParams(
            collective_id=0, has_side_effects=True, vmem_limit_bytes=56 * 1024 * 1024
        ),
    )(*(pltpu.with_memory_space_constraint(a, pltpu.HBM) for a in (
        target, source, cotangent, target_gain.reshape(1, width), source_gain.reshape(1, width),
        w_query, w_key, w_value, w_out,
    )))
    return pl.pallas_call(
        write_out,
        out_shape=tuple(jax.ShapeDtypeStruct(m.shape, m.dtype) for m in made),
        in_specs=[vm_spec] * 3,
        out_specs=(pl.BlockSpec(memory_space=pltpu.HBM),) * 3,
        scratch_shapes=[sem((3,))],
        compiler_params=pltpu.CompilerParams(vmem_limit_bytes=1024 * 1024),
    )(*made)


def solution(mesh, ny=4, nx=4):
    nz = mesh.shape["tp"] // 2
    split = Mesh(mesh.devices.reshape(ny, nx, nz, 2), ("y", "x", "z", "c"))
    sp, tp, every = ("y", "x"), ("z", "c"), ("y", "x", "z", "c")
    in_specs = (P(sp, None), P(sp, None), P(sp, None), P(), P(), P(None, tp), P(), P(), P(tp, None))
    out_specs = (P(every, None), P(every, None), P(tp, sp))
    return jax.shard_map(
        functools.partial(on_device, (ny, nx, nz)),
        mesh=split, in_specs=in_specs, out_specs=out_specs, check_vma=False,
    )
```

```python
import functools
import math

import jax
import jax.numpy as jnp
from jax import lax
from jax.experimental import pallas as pl
from jax.experimental.pallas import tpu as pltpu
from jax.sharding import Mesh
from jax.sharding import PartitionSpec as P

HEAD = 128
NORM_EPS = 1e-06
INV_ROOT = HEAD ** (-0.5)
LOG2E = math.log2(math.e)
F32, BF16 = jnp.float32, jnp.bfloat16
NN = (((1,), (0,)), ((), ()))
NT = (((1,), (1,)), ((), ()))
TN = (((0,), (0,)), ((), ()))
SHAPE = {"y": 4, "x": 4, "c": 2}


def dot(a, b, dims):
    return lax.dot_general(a, b, dims, preferred_element_type=F32)


def norm_rows(src, dst, gain):
    rows, step = src.shape[0], 16

    def one(k, carry):
        at = pl.ds(pl.multiple_of(k * step, step), step)
        v = src[at, :].astype(F32)
        r = lax.rsqrt(jnp.mean(v * v, axis=1, keepdims=True) + NORM_EPS)
        dst[at, :] = (v * r * gain[...]).astype(BF16)
        return carry

    lax.fori_loop(0, rows // step, one, 0, unroll=4)


def norm_back(rows, gain, upstream):
    r = lax.rsqrt(jnp.mean(rows * rows, axis=1, keepdims=True) + NORM_EPS)
    unit = rows * r
    pulled = upstream * gain
    return (r * (pulled - unit * jnp.mean(pulled * unit, axis=1, keepdims=True))).astype(BF16)


def wait_bytes(ref, sem):
    pltpu.make_async_copy(ref, ref, sem).wait()


def kernel(
    dims, tgt_h, src_h, cot_h, tg_h, sg_h, wq_h, wk_h, wv_h, wo_h,
    gt_o, gs_o, go_o,
    srcb, swin, sn, tgtb, twin, tn, cotb, tgb, sgb, wkv, wob,
    kv, qg, est, pgt, lhs, t_b, rhs, stat, aw, tk,
    ys, yr, gkv, ps, pr, xs, xr, xown, zk, zr,
    wq4, gqo, gqi, pmat, ts, tr, gos, gor,
    ld, kv_r, kvp_r, qg_r, st_r, y_r, ps_r, x_r, zk_r, wq_r, gq_r, t_r, go_r,
    kv_s, kvp_s, qg_s, st_s, y_s, ps_s, x_s, zk_s, wq_s, gq_s, t_s, go_s,
    up_1, up_2, up_4, seen_x, seen_y,
):
    ny, nx, nz, gsz, rt, rs, win = dims
    ns = ny * nx
    y, x, z, c = (lax.axis_index(a) for a in ("y", "x", "z", "c"))
    o = 1 - c
    s_me = y * nx + x
    zo = z + 1 - 2 * lax.rem(z, 2)
    zf = lax.rem(z - 1 + 2 * lax.rem(z, 2) + nz, nz)
    hz = lax.rem(z, 2)
    mem = 2 * hz + c
    zp = lax.select(c == 0, zo, zf)
    half = kv.shape[2]
    rows = tgtb.shape[0]
    width = tgtb.shape[1]

    barrier = pltpu.get_barrier_semaphore()

    def signal(sem, to):
        pl.semaphore_signal(sem, inc=1, device_id=to, device_id_type=pl.DeviceIdType.MESH)

    def beside(k):
        return [lax.rem(z + k, nz), lax.rem(z + nz - k, nz)] if 2 * k < nz else [lax.rem(z + k, nz)]

    peers = [{"c": o}]
    x_peers = [{"x": lax.rem(x + dx, nx)} for dx in range(1, nx)]
    y_peers = [{"y": lax.rem(y + dy, ny)} for dy in range(1, ny)]
    peers.extend(x_peers + y_peers)
    for pz in [zo, zf] if nz > 2 else [zo]:
        peers.extend([{"z": pz, "c": c}, {"z": pz, "c": o}])
    for peer in peers:
        signal(barrier, peer)

    def load(k, a, b):
        d = pltpu.make_async_copy(a, b, ld.at[k])
        d.start()
        return d

    t_me = 2 * z + c
    w0 = pl.multiple_of(lax.div(rs * t_me, 8) * 8, 8)
    l_tgt = load(4, tgt_h, tgtb)
    l_tg = load(5, tg_h, tgb)
    l_wq = load(6, wq_h, wq4.at[mem])
    l_cot = load(7, cot_h, cotb)
    l_wo = load(8, wo_h, wob)
    l_src = load(0, src_h.at[pl.ds(pl.multiple_of(c * half, half), half), :], srcb)
    l_sg = load(1, sg_h, sgb)
    l_wk = load(2, wk_h, wkv.at[:, pl.ds(0, HEAD)])
    l_wv = load(3, wv_h, wkv.at[:, pl.ds(HEAD, HEAD)])
    l_swin = load(9, src_h.at[pl.ds(w0, win), :], swin)
    l_twin = load(10, tgt_h.at[pl.ds(pl.multiple_of(2 * rt * z, 2 * rt), 2 * rt), :], twin)

    def send(a, b, s_sem, r_sem, to):
        d = pltpu.make_async_remote_copy(
            src_ref=a, dst_ref=b, send_sem=s_sem, recv_sem=r_sem,
            device_id=to, device_id_type=pl.DeviceIdType.MESH,
        )
        d.start()
        return d

    l_tgt.wait()
    l_tg.wait()
    norm_rows(tgtb, tn, tgb)
    l_wq.wait()
    qg[0, :, pl.ds(0, HEAD)] = dot(tn[...], wq4[mem], NN).astype(BF16)
    l_cot.wait()
    l_wo.wait()
    qg[0, :, pl.ds(HEAD, HEAD)] = dot(cotb[...], wob[...], NT).astype(BF16)
    pl.semaphore_wait(barrier, len(peers))
    sends = []
    x_order = [d for d in (1, 3, 2) if d < nx]
    y_order = [d for d in (2, 1, 3) if d < ny]
    for d in y_order:
        sends.append(send(qg.at[0], qg.at[d], qg_s.at[d], qg_r.at[d], {"y": lax.rem(y + d, ny)}))
    for peer in y_peers:
        signal(seen_y, peer)
    for peer in x_peers:
        signal(seen_x, peer)
    for pz in beside(1):
        signal(up_1, {"z": pz})
    sends.append(send(wq4.at[mem], wq4.at[mem], wq_s.at[0], wq_r.at[0], {"z": zo}))
    sends.append(send(wq4.at[mem], wq4.at[mem], wq_s.at[1], wq_r.at[1], {"c": o}))
    l_src.wait()
    l_sg.wait()
    norm_rows(srcb, sn, sgb)
    l_wk.wait()
    l_wv.wait()
    kv[0, c] = dot(sn[...], wkv[...], NN).astype(BF16)
    for d in x_order:
        sends.append(send(kv.at[0, c], kv.at[d, c], kv_s.at[d], kv_r.at[d], {"x": lax.rem(x + d, nx)}))
    sends.append(send(kv.at[0, c], kv.at[0, c], kvp_s.at[0], kvp_r.at[0], {"c": o}))
    pl.semaphore_wait(up_1, len(beside(1)))
    for pz in beside(2):
        signal(up_2, {"z": pz})

    for d in range(1, ny):
        wait_bytes(qg.at[d], qg_r.at[d])
    pl.semaphore_wait(up_2, len(beside(2)))
    for pz in beside(4):
        signal(up_4, {"z": pz})
    q_all = qg[:, :, pl.ds(0, HEAD)].reshape(ny * rows, HEAD)
    g_all = qg[:, :, pl.ds(HEAD, HEAD)].reshape(ny * rows, HEAD)
    tot = jnp.zeros((1, ny * rows), F32)
    tilt = jnp.zeros((1, ny * rows), F32)

    def unit(d, h, tot, tilt):
        key, val = kv[d, h, :, pl.ds(0, HEAD)], kv[d, h, :, pl.ds(HEAD, HEAD)]
        e = jnp.exp2(dot(key, q_all, NT) * (INV_ROOT * LOG2E))
        g = dot(val, g_all, NT)
        t = e * g
        est[d, h] = e
        pgt[d, h] = g
        lhs[1, d, h] = e.astype(BF16)
        t_b[d, h] = t.astype(BF16)
        return tot + jnp.sum(e, axis=0, keepdims=True), tilt + jnp.sum(t, axis=0, keepdims=True)

    def unit_sums(d, h, first):
        both = dot(kv[d, h], lhs[1, d, h], TN)
        one = dot(kv[d, h, :, pl.ds(0, HEAD)], t_b[d, h], TN)
        aw[...] = both if first else aw[...] + both
        tk[...] = one if first else tk[...] + one

    x_seen = [d for d in (1, 3, 2) if d < nx]
    tot, tilt = unit(0, c, tot, tilt)
    before = 0
    for d in x_seen:
        wait_bytes(kv.at[d, c], kv_r.at[d])
        sends.append(send(kv.at[d, c], kv.at[d, c], kvp_s.at[d], kvp_r.at[d], {"c": o}))
        wait_bytes(kv.at[before, o], kvp_r.at[before])
        tot, tilt = unit(before, o, tot, tilt)
        tot, tilt = unit(d, c, tot, tilt)
        before = d
    wait_bytes(kv.at[before, o], kvp_r.at[before])
    tot, tilt = unit(before, o, tot, tilt)

    for e in range(ny):
        stat[0, e, 0:1, :] = tot[:, e * rows:(e + 1) * rows]
        stat[0, e, 1:2, :] = tilt[:, e * rows:(e + 1) * rows]
    for d in y_order:
        sends.append(send(stat.at[0], stat.at[d], st_s.at[d], st_r.at[d], {"y": lax.rem(y + d, ny)}))
    for d in range(nx):
        for h in range(2):
            unit_sums(d, h, d + h == 0)
    for e in y_order:
        ys[e] = aw[pl.ds(HEAD, HEAD), pl.ds(e * rows, rows)].astype(BF16)
        sends.append(send(ys.at[e], yr.at[e], y_s.at[e], y_r.at[e], {"y": lax.rem(y + ny - e, ny)}))
    for d in range(1, ny):
        wait_bytes(stat.at[d], st_r.at[d])
    tots, deltas = [], []
    for e in range(ny):
        both = stat[0, e]
        for d in range(1, ny):
            both = both + stat[d, (e - d) % ny]
        tots.append(1.0 / both[0:1, :])
        deltas.append(both[1:2, :] / both[0:1, :])
    inv_total = jnp.concatenate(tots, axis=1)
    delta = jnp.concatenate(deltas, axis=1)

    pl.semaphore_wait(seen_y, len(y_peers))
    gq = ((tk[...] - delta * aw[pl.ds(0, HEAD), :]) * (inv_total * INV_ROOT)).T.astype(BF16)
    quarter = rows // 4
    for e in range(ny):
        for k in range(4):
            gqo[4 * e + k] = gq[e * rows + k * quarter:e * rows + (k + 1) * quarter, :]
    for e in y_order + [0]:
        py = lax.rem(y + ny - e, ny)
        for step in (2, 3, 1, 0):
            if e or step:
                pz = zo if step > 1 else z
                pc = o if step % 2 else c
                to = 2 * lax.rem(pz, 2) + pc
                send(gqo.at[4 * e + to], gqi.at[4 * e + mem], gq_s, gq_r, {"y": py, "z": pz, "c": pc})
    gqi[mem] = gqo[mem]
    pl.semaphore_wait(seen_x, len(x_peers))
    scale = jnp.broadcast_to(inv_total, (8, ny * rows)).T[:, 0:1]
    rhs[0] = (q_all.astype(F32) * (scale * INV_ROOT)).astype(BF16)
    rhs[1] = (g_all.astype(F32) * scale).astype(BF16)
    order = [d for d in (2, 1, 3, 0) if d < nx]

    def other(d):
        for h in range(2):
            lhs[0, d, h] = (est[d, h] * (pgt[d, h] - delta)).astype(BF16)
            ps[d, pl.ds(h * half, half), :] = dot(lhs[o, d, h], rhs[o], NN).astype(BF16)
        sends.append(send(ps.at[d], pr.at[d], ps_s.at[d], ps_r.at[d], {"c": o}))

    def own(d):
        for h in range(2):
            gkv[d, pl.ds(h * half, half), :] = dot(lhs[c, d, h], rhs[c], NN)

    def pass_on(d):
        wait_bytes(pr.at[d], ps_r.at[d])
        mine = gkv[d] + pr[d].astype(F32)
        mine = mine.reshape(nz // 2, 2, 2 * rs, HEAD)
        px = lax.rem(x + nx - d, nx)
        for h in range(2):
            if d == 0:
                xown[h] = mine[:, h]
            xs[d, h] = mine[:, h].astype(BF16)
        sends.append(send(xs.at[d, 1 - hz], xr.at[d, 1], x_s.at[d, 1], x_r.at[d, 1], {"x": px, "z": zp}))
        if d:
            sends.append(send(xs.at[d, hz], xr.at[d, 0], x_s.at[d, 0], x_r.at[d, 0], {"x": px}))

    steps = [(other, order[0])]
    for i in range(len(order)):
        if i + 1 < len(order):
            steps.append((other, order[i + 1]))
        steps.append((own, order[i]))
        if i:
            steps.append((pass_on, order[i - 1]))
    for step, d in steps[:5]:
        step(d)
    wait_bytes(wq4.at[0], wq_r.at[0])
    mem_z = 2 * lax.rem(zo, 2) + c
    sends.append(send(wq4.at[mem_z], wq4.at[mem_z], wq_s.at[2], wq_r.at[2], {"c": o}))
    for step, d in steps[5:]:
        step(d)
    pass_on(order[-1])
    wait_bytes(gqi.at[pl.ds(0, 4 * ny - 1)], gq_r)
    wait_bytes(wq4.at[0], wq_r.at[1])
    wait_bytes(wq4.at[0], wq_r.at[2])
    up = None
    for k in range(4):
        one = gqi[k].astype(F32)
        for e in range(1, ny):
            one = one + gqi[4 * e + k].astype(F32)
        one = dot(one.astype(BF16), wq4[k], NT)
        up = one if up is None else up + one
    pmat[...] = up
    pieces = quarter // rt
    for k in range(pieces):
        ts[k] = pmat[pl.ds(rt * k, rt), :].astype(BF16)
    pl.semaphore_wait(up_4, len(beside(4)))
    pair = lax.div(z, 2)
    per = pieces // 2
    for k in range(pieces):
        pz, pc = per * mem + k // 2, k % 2
        mine = jnp.logical_and(pz == z, pc == c)

        @pl.when(jnp.logical_not(mine))
        def _():
            send(ts.at[k], tr.at[pair], t_s, t_r, {"z": pz, "c": pc})

        @pl.when(mine)
        def _():
            tr[pair] = ts[k]

    far = sorted(range(1, nz), key=lambda k: -min(k, nz - k))

    ksum = xown[hz]
    for d in range(nx):
        for h in range(2):
            if d or h:
                wait_bytes(xr.at[d, h], x_r.at[d, h])
                ksum = ksum + xr[d, h].astype(F32)
    for k in range(nz // 2):
        for cc in range(2):
            zk[2 * k + cc] = ksum[k, rs * cc:rs * cc + rs, :].reshape(rs // 4, 4, HEAD).astype(BF16)
    slot = 2 * lax.div(z, 2) + c
    for dz in sorted(range(0, nz, 2), key=lambda k: -min(k, nz - k)):
        pz = lax.rem(z + dz, nz)
        for cc in (c, o):
            if dz or cc is o:
                send(zk.at[2 * lax.div(pz, 2) + cc], zr.at[slot], zk_s, zk_r, {"z": pz, "c": cc})
    zr[slot] = zk[slot]

    for e in range(1, ny):
        wait_bytes(yr.at[e], y_r.at[e])
    av = aw[pl.ds(HEAD, HEAD), pl.ds(0, rows)]
    for e in range(1, ny):
        av = av + yr[e].astype(F32)
    go = dot((av * tots[0]).astype(BF16), cotb[...], NN)
    wc = width // ns
    for k in range(ns):
        gos[k] = go[:, k * wc:(k + 1) * wc].astype(BF16)
    for dy in (2, 1, 3, 0):
        for dx in (2, 1, 3, 0):
            if dy < ny and dx < nx and (dy or dx):
                py, px = lax.rem(y + dy, ny), lax.rem(x + dx, nx)
                send(gos.at[py * nx + px], gor.at[s_me], go_s, go_r, {"y": py, "x": px})
    gor[s_me] = gos[s_me]

    l_swin.wait()
    row_at = lax.broadcasted_iota(jnp.int32, (rs, win), 0) + (rs * t_me - w0)
    pick = (lax.broadcasted_iota(jnp.int32, (rs, win), 1) == row_at).astype(F32).astype(BF16)
    sw = dot(pick, swin[...], NN)
    l_twin.wait()
    own_piece = mem == lax.div(z, per)

    @pl.when(own_piece)
    def _():
        wait_bytes(tr.at[pl.ds(0, nz // 2 - 1)], t_r)
        wait_bytes(ts.at[pl.ds(0, pieces - 1)], t_s)

    @pl.when(jnp.logical_not(own_piece))
    def _():
        wait_bytes(tr, t_r)
        wait_bytes(ts, t_s)

    up = jnp.sum(tr[...].astype(F32), axis=0)
    tw = twin[...].astype(F32)
    tw = jnp.where(c == 0, tw[0:rt, :], tw[rt:2 * rt, :])
    gt_o[...] = norm_back(tw, tgb[...], up)

    wait_bytes(gor.at[pl.ds(0, ns - 1)], go_r)
    go_o[...] = jnp.sum(gor[...].astype(F32), axis=0).astype(BF16)

    wait_bytes(zr.at[pl.ds(0, nz - 1)], zk_r)
    both = [zr[0].astype(F32), zr[1].astype(F32)]
    for k in range(2, nz):
        both[k % 2] = both[k % 2] + zr[k].astype(F32)
    both = jnp.concatenate([one.reshape(rs, HEAD) for one in both], axis=1).astype(BF16)
    gs_o[...] = norm_back(sw, sgb[...], dot(both, wkv[...], NT))

    for d in sends:
        d.wait_send()
    wait_bytes(gos.at[pl.ds(0, ns - 1)], go_s)
    wait_bytes(gqo.at[pl.ds(0, 4 * ny - 1)], gq_s)
    wait_bytes(zk.at[pl.ds(0, nz - 1)], zk_s)


def write_out(a, b, c, a_o, b_o, c_o, sems):
    copies = [pltpu.make_async_copy(i, j, sems.at[k]) for k, (i, j) in enumerate(((a, a_o), (b, b_o), (c, c_o)))]
    for one in copies:
        one.start()
    for one in copies:
        one.wait()


def on_device(shape, target, source, cotangent, target_gain, source_gain, w_query, w_key, w_value, w_out):
    ny, nx, nz = shape
    rows, width = target.shape
    srows = source.shape[0]
    half = srows // 2
    rt, rs = rows // (2 * nz), srows // (2 * nz)
    win = rs if rs % 8 == 0 else rs + 4
    ns = ny * nx
    wide = ny * rows
    vm = pltpu.VMEM
    sem = pltpu.SemaphoreType.DMA
    scratch = [
        vm((half, width), BF16), vm((win, width), BF16), vm((half, width), BF16),
        vm((rows, width), BF16), vm((2 * rt, width), BF16), vm((rows, width), BF16),
        vm((rows, width), BF16), vm((1, width), F32), vm((1, width), F32),
        vm((width, 2 * HEAD), BF16), vm((HEAD, width), BF16),
        vm((nx, 2, half, 2 * HEAD), BF16), vm((ny, rows, 2 * HEAD), BF16),
        vm((nx, 2, half, wide), F32), vm((nx, 2, half, wide), F32),
        vm((2, nx, 2, half, wide), BF16), vm((nx, 2, half, wide), BF16), vm((2, wide, HEAD), BF16),
        vm((ny, ny, 2, rows), F32), vm((2 * HEAD, wide), F32), vm((HEAD, wide), F32),
        vm((ny, HEAD, rows), BF16), vm((ny, HEAD, rows), BF16),
        vm((nx, srows, HEAD), F32), vm((nx, srows, HEAD), BF16), vm((nx, srows, HEAD), BF16),
        vm((nx, 2, nz // 2, 2 * rs, HEAD), BF16), vm((nx, 2, nz // 2, 2 * rs, HEAD), BF16),
        vm((2, nz // 2, 2 * rs, HEAD), F32), vm((nz, rs // 4, 4, HEAD), BF16), vm((nz, rs // 4, 4, HEAD), BF16),
        vm((4, width, HEAD), BF16), vm((4 * ny, rows // 4, HEAD), BF16), vm((4 * ny, rows // 4, HEAD), BF16),
        vm((rows // 4, width), F32), vm((rows // 4 // rt, rt, width), BF16), vm((nz // 2, rt, width), BF16),
        vm((ns, HEAD, width // ns), BF16), vm((ns, HEAD, width // ns), BF16),
        sem((11,)), sem((nx,)), sem((nx,)), sem((ny,)), sem((ny,)), sem((ny,)), sem((nx,)), sem((nx, 2)),
        sem, sem((3,)), sem, sem, sem,
        sem((nx,)), sem((nx,)), sem((ny,)), sem((ny,)), sem((ny,)), sem((nx,)), sem((nx, 2)),
        sem, sem((3,)), sem, sem, sem,
        pltpu.SemaphoreType.REGULAR, pltpu.SemaphoreType.REGULAR, pltpu.SemaphoreType.REGULAR,
        pltpu.SemaphoreType.REGULAR, pltpu.SemaphoreType.REGULAR,
    ]
    any_spec = pl.BlockSpec(memory_space=pltpu.HBM)
    vm_spec = pl.BlockSpec(memory_space=pltpu.VMEM)
    made = pl.pallas_call(
        functools.partial(kernel, (ny, nx, nz, 0, rt, rs, win)),
        out_shape=(
            vm((rt, width), BF16), vm((rs, width), BF16), vm((HEAD, width // ns), BF16),
        ),
        in_specs=[any_spec] * 9,
        out_specs=(vm_spec,) * 3,
        scratch_shapes=scratch,
        compiler_params=pltpu.CompilerParams(
            collective_id=0, has_side_effects=True, vmem_limit_bytes=56 * 1024 * 1024
        ),
    )(*(pltpu.with_memory_space_constraint(a, pltpu.HBM) for a in (
        target, source, cotangent, target_gain.reshape(1, width), source_gain.reshape(1, width),
        w_query, w_key, w_value, w_out,
    )))
    return pl.pallas_call(
        write_out,
        out_shape=tuple(jax.ShapeDtypeStruct(m.shape, m.dtype) for m in made),
        in_specs=[vm_spec] * 3,
        out_specs=(pl.BlockSpec(memory_space=pltpu.HBM),) * 3,
        scratch_shapes=[sem((3,))],
        compiler_params=pltpu.CompilerParams(vmem_limit_bytes=1024 * 1024),
    )(*made)


def solution(mesh, ny=4, nx=4):
    nz = mesh.shape["tp"] // 2
    split = Mesh(mesh.devices.reshape(ny, nx, nz, 2), ("y", "x", "z", "c"))
    sp, tp, every = ("y", "x"), ("z", "c"), ("y", "x", "z", "c")
    in_specs = (P(sp, None), P(sp, None), P(sp, None), P(), P(), P(None, tp), P(), P(), P(tp, None))
    out_specs = (P(every, None), P(every, None), P(tp, sp))
    return jax.shard_map(
        functools.partial(on_device, (ny, nx, nz)),
        mesh=split, in_specs=in_specs, out_specs=out_specs, check_vma=False,
    )
```

```python
import functools
import math

import jax
import jax.numpy as jnp
from jax import lax
from jax.experimental import pallas as pl
from jax.experimental.pallas import tpu as pltpu
from jax.sharding import Mesh
from jax.sharding import PartitionSpec as P

HEAD = 128
NORM_EPS = 1e-06
INV_ROOT = HEAD ** (-0.5)
LOG2E = math.log2(math.e)
F32, BF16 = jnp.float32, jnp.bfloat16
NN = (((1,), (0,)), ((), ()))
NT = (((1,), (1,)), ((), ()))
TN = (((0,), (0,)), ((), ()))
SHAPE = {"y": 4, "x": 4, "c": 2}


def dot(a, b, dims):
    return lax.dot_general(a, b, dims, preferred_element_type=F32)


def norm_rows(src, dst, gain):
    rows, step = src.shape[0], 16

    def one(k, carry):
        at = pl.ds(pl.multiple_of(k * step, step), step)
        v = src[at, :].astype(F32)
        r = lax.rsqrt(jnp.mean(v * v, axis=1, keepdims=True) + NORM_EPS)
        dst[at, :] = (v * r * gain[...]).astype(BF16)
        return carry

    lax.fori_loop(0, rows // step, one, 0, unroll=4)


def norm_back(rows, gain, upstream):
    r = lax.rsqrt(jnp.mean(rows * rows, axis=1, keepdims=True) + NORM_EPS)
    unit = rows * r
    pulled = upstream * gain
    return (r * (pulled - unit * jnp.mean(pulled * unit, axis=1, keepdims=True))).astype(BF16)


def wait_bytes(ref, sem):
    pltpu.make_async_copy(ref, ref, sem).wait()


def kernel(
    dims, tgt_h, src_h, cot_h, tg_h, sg_h, wq_h, wk_h, wv_h, wo_h,
    gt_o, gs_o, go_o,
    srcb, swin, sn, tgtb, twin, tn, cotb, tgb, sgb, wkv, wob,
    kv, qg, est, pgt, lhs, t_b, rhs, stat, aw, tk,
    ys, yr, gkv, ps, pr, xs, xr, xown, zk, zr,
    wq4, gqo, gqi, pmat, ts, tr, gos, gor,
    ld, kv_r, kvp_r, qg_r, st_r, y_r, ps_r, x_r, zk_r, wq_r, gq_r, t_r, go_r,
    kv_s, kvp_s, qg_s, st_s, y_s, ps_s, x_s, zk_s, wq_s, gq_s, t_s, go_s,
    up_1, up_2, up_4, seen_x, seen_y,
):
    ny, nx, nz, gsz, rt, rs, win = dims
    ns = ny * nx
    y, x, z, c = (lax.axis_index(a) for a in ("y", "x", "z", "c"))
    o = 1 - c
    s_me = y * nx + x
    zo = z + 1 - 2 * lax.rem(z, 2)
    zf = lax.rem(z - 1 + 2 * lax.rem(z, 2) + nz, nz)
    hz = lax.rem(z, 2)
    mem = 2 * hz + c
    zp = lax.select(c == 0, zo, zf)
    half = kv.shape[2]
    rows = tgtb.shape[0]
    width = tgtb.shape[1]

    barrier = pltpu.get_barrier_semaphore()

    def signal(sem, to):
        pl.semaphore_signal(sem, inc=1, device_id=to, device_id_type=pl.DeviceIdType.MESH)

    def beside(k):
        return [lax.rem(z + k, nz), lax.rem(z + nz - k, nz)] if 2 * k < nz else [lax.rem(z + k, nz)]

    peers = [{"c": o}]
    x_peers = [{"x": lax.rem(x + dx, nx)} for dx in range(1, nx)]
    y_peers = [{"y": lax.rem(y + dy, ny)} for dy in range(1, ny)]
    peers.extend(x_peers + y_peers)
    for pz in [zo, zf] if nz > 2 else [zo]:
        peers.extend([{"z": pz, "c": c}, {"z": pz, "c": o}])
    for peer in peers:
        signal(barrier, peer)

    def load(k, a, b):
        d = pltpu.make_async_copy(a, b, ld.at[k])
        d.start()
        return d

    t_me = 2 * z + c
    w0 = pl.multiple_of(lax.div(rs * t_me, 8) * 8, 8)
    l_tgt = load(4, tgt_h, tgtb)
    l_tg = load(5, tg_h, tgb)
    l_wq = load(6, wq_h, wq4.at[mem])
    l_cot = load(7, cot_h, cotb)
    l_wo = load(8, wo_h, wob)
    l_src = load(0, src_h.at[pl.ds(pl.multiple_of(c * half, half), half), :], srcb)
    l_sg = load(1, sg_h, sgb)
    l_wk = load(2, wk_h, wkv.at[:, pl.ds(0, HEAD)])
    l_wv = load(3, wv_h, wkv.at[:, pl.ds(HEAD, HEAD)])
    l_swin = load(9, src_h.at[pl.ds(w0, win), :], swin)
    l_twin = load(10, tgt_h.at[pl.ds(pl.multiple_of(2 * rt * z, 2 * rt), 2 * rt), :], twin)

    def send(a, b, s_sem, r_sem, to):
        d = pltpu.make_async_remote_copy(
            src_ref=a, dst_ref=b, send_sem=s_sem, recv_sem=r_sem,
            device_id=to, device_id_type=pl.DeviceIdType.MESH,
        )
        d.start()
        return d

    l_tgt.wait()
    l_tg.wait()
    norm_rows(tgtb, tn, tgb)
    l_wq.wait()
    qg[0, :, pl.ds(0, HEAD)] = dot(tn[...], wq4[mem], NN).astype(BF16)
    l_cot.wait()
    l_wo.wait()
    qg[0, :, pl.ds(HEAD, HEAD)] = dot(cotb[...], wob[...], NT).astype(BF16)
    pl.semaphore_wait(barrier, len(peers))
    sends = []
    x_order = [d for d in (1, 3, 2) if d < nx]
    y_order = [d for d in (2, 1, 3) if d < ny]
    for d in y_order:
        sends.append(send(qg.at[0], qg.at[d], qg_s.at[d], qg_r.at[d], {"y": lax.rem(y + d, ny)}))
    for peer in y_peers:
        signal(seen_y, peer)
    for peer in x_peers:
        signal(seen_x, peer)
    for pz in beside(1):
        signal(up_1, {"z": pz})
    sends.append(send(wq4.at[mem], wq4.at[mem], wq_s.at[0], wq_r.at[0], {"z": zo}))
    sends.append(send(wq4.at[mem], wq4.at[mem], wq_s.at[1], wq_r.at[1], {"c": o}))
    l_src.wait()
    l_sg.wait()
    norm_rows(srcb, sn, sgb)
    l_wk.wait()
    l_wv.wait()
    kv[0, c] = dot(sn[...], wkv[...], NN).astype(BF16)
    for d in x_order:
        sends.append(send(kv.at[0, c], kv.at[d, c], kv_s.at[d], kv_r.at[d], {"x": lax.rem(x + d, nx)}))
    sends.append(send(kv.at[0, c], kv.at[0, c], kvp_s.at[0], kvp_r.at[0], {"c": o}))
    pl.semaphore_wait(up_1, len(beside(1)))
    for pz in beside(2):
        signal(up_2, {"z": pz})

    for d in range(1, ny):
        wait_bytes(qg.at[d], qg_r.at[d])
    pl.semaphore_wait(up_2, len(beside(2)))
    for pz in beside(4):
        signal(up_4, {"z": pz})
    q_all = qg[:, :, pl.ds(0, HEAD)].reshape(ny * rows, HEAD)
    g_all = qg[:, :, pl.ds(HEAD, HEAD)].reshape(ny * rows, HEAD)
    tot = jnp.zeros((1, ny * rows), F32)
    tilt = jnp.zeros((1, ny * rows), F32)

    def unit(d, h, tot, tilt):
        key, val = kv[d, h, :, pl.ds(0, HEAD)], kv[d, h, :, pl.ds(HEAD, HEAD)]
        e = jnp.exp2(dot(key, q_all, NT) * (INV_ROOT * LOG2E) - 2.0)
        g = dot(val, g_all, NT)
        t = e * g
        est[d, h] = e
        pgt[d, h] = g
        lhs[1, d, h] = e.astype(BF16)
        t_b[d, h] = t.astype(BF16)
        return tot + jnp.sum(e, axis=0, keepdims=True), tilt + jnp.sum(t, axis=0, keepdims=True)

    def unit_sums(d, h, first):
        both = dot(kv[d, h], lhs[1, d, h], TN)
        one = dot(kv[d, h, :, pl.ds(0, HEAD)], t_b[d, h], TN)
        aw[...] = both if first else aw[...] + both
        tk[...] = one if first else tk[...] + one

    x_seen = [d for d in (1, 3, 2) if d < nx]
    tot, tilt = unit(0, c, tot, tilt)
    before = 0
    for d in x_seen:
        wait_bytes(kv.at[d, c], kv_r.at[d])
        sends.append(send(kv.at[d, c], kv.at[d, c], kvp_s.at[d], kvp_r.at[d], {"c": o}))
        wait_bytes(kv.at[before, o], kvp_r.at[before])
        tot, tilt = unit(before, o, tot, tilt)
        tot, tilt = unit(d, c, tot, tilt)
        before = d
    wait_bytes(kv.at[before, o], kvp_r.at[before])
    tot, tilt = unit(before, o, tot, tilt)

    for e in range(ny):
        stat[0, e, 0:1, :] = tot[:, e * rows:(e + 1) * rows]
        stat[0, e, 1:2, :] = tilt[:, e * rows:(e + 1) * rows]
    for d in y_order:
        sends.append(send(stat.at[0], stat.at[d], st_s.at[d], st_r.at[d], {"y": lax.rem(y + d, ny)}))
    for d in range(nx):
        for h in range(2):
            unit_sums(d, h, d + h == 0)
    for e in y_order:
        ys[e] = aw[pl.ds(HEAD, HEAD), pl.ds(e * rows, rows)].astype(BF16)
        sends.append(send(ys.at[e], yr.at[e], y_s.at[e], y_r.at[e], {"y": lax.rem(y + ny - e, ny)}))
    for d in range(1, ny):
        wait_bytes(stat.at[d], st_r.at[d])
    tots, deltas = [], []
    for e in range(ny):
        both = stat[0, e]
        for d in range(1, ny):
            both = both + stat[d, (e - d) % ny]
        tots.append(1.0 / both[0:1, :])
        deltas.append(both[1:2, :] / both[0:1, :])
    inv_total = jnp.concatenate(tots, axis=1)
    delta = jnp.concatenate(deltas, axis=1)

    pl.semaphore_wait(seen_y, len(y_peers))
    gq = ((tk[...] - delta * aw[pl.ds(0, HEAD), :]) * (inv_total * INV_ROOT)).T.astype(BF16)
    quarter = rows // 4
    for e in range(ny):
        for k in range(4):
            gqo[4 * e + k] = gq[e * rows + k * quarter:e * rows + (k + 1) * quarter, :]
    for e in y_order + [0]:
        py = lax.rem(y + ny - e, ny)
        for step in (2, 3, 1, 0):
            if e or step:
                pz = zo if step > 1 else z
                pc = o if step % 2 else c
                to = 2 * lax.rem(pz, 2) + pc
                send(gqo.at[4 * e + to], gqi.at[4 * e + mem], gq_s, gq_r, {"y": py, "z": pz, "c": pc})
    gqi[mem] = gqo[mem]
    pl.semaphore_wait(seen_x, len(x_peers))
    rhs[0] = q_all
    rhs[1] = g_all
    root = lax.select(c == 0, jnp.float32(INV_ROOT), jnp.float32(1.0))
    root_o = lax.select(c == 0, jnp.float32(1.0), jnp.float32(INV_ROOT))
    order = [d for d in (2, 1, 3, 0) if d < nx]

    def other(d):
        for h in range(2):
            p = est[d, h] * inv_total
            lhs[0, d, h] = (p * (pgt[d, h] - delta)).astype(BF16)
            lhs[1, d, h] = p.astype(BF16)
            ps[d, pl.ds(h * half, half), :] = (dot(lhs[o, d, h], rhs[o], NN) * root_o).astype(BF16)
        sends.append(send(ps.at[d], pr.at[d], ps_s.at[d], ps_r.at[d], {"c": o}))

    def own(d):
        for h in range(2):
            gkv[d, pl.ds(h * half, half), :] = dot(lhs[c, d, h], rhs[c], NN) * root

    def pass_on(d):
        wait_bytes(pr.at[d], ps_r.at[d])
        mine = gkv[d] + pr[d].astype(F32)
        mine = mine.reshape(nz // 2, 2, 2 * rs, HEAD)
        px = lax.rem(x + nx - d, nx)
        for h in range(2):
            if d == 0:
                xown[h] = mine[:, h]
            xs[d, h] = mine[:, h].astype(BF16)
        sends.append(send(xs.at[d, 1 - hz], xr.at[d, 1], x_s.at[d, 1], x_r.at[d, 1], {"x": px, "z": zp}))
        if d:
            sends.append(send(xs.at[d, hz], xr.at[d, 0], x_s.at[d, 0], x_r.at[d, 0], {"x": px}))

    steps = [(other, order[0])]
    for i in range(len(order)):
        if i + 1 < len(order):
            steps.append((other, order[i + 1]))
        steps.append((own, order[i]))
        if i:
            steps.append((pass_on, order[i - 1]))
    for step, d in steps[:5]:
        step(d)
    wait_bytes(wq4.at[0], wq_r.at[0])
    mem_z = 2 * lax.rem(zo, 2) + c
    sends.append(send(wq4.at[mem_z], wq4.at[mem_z], wq_s.at[2], wq_r.at[2], {"c": o}))
    for step, d in steps[5:]:
        step(d)
    pass_on(order[-1])
    wait_bytes(gqi.at[pl.ds(0, 4 * ny - 1)], gq_r)
    wait_bytes(wq4.at[0], wq_r.at[1])
    wait_bytes(wq4.at[0], wq_r.at[2])
    up = None
    for k in range(4):
        one = gqi[k].astype(F32)
        for e in range(1, ny):
            one = one + gqi[4 * e + k].astype(F32)
        one = dot(one.astype(BF16), wq4[k], NT)
        up = one if up is None else up + one
    pmat[...] = up
    pieces = quarter // rt
    for k in range(pieces):
        ts[k] = pmat[pl.ds(rt * k, rt), :].astype(BF16)
    pl.semaphore_wait(up_4, len(beside(4)))
    pair = lax.div(z, 2)
    per = pieces // 2
    for k in range(pieces):
        pz, pc = per * mem + k // 2, k % 2
        mine = jnp.logical_and(pz == z, pc == c)

        @pl.when(jnp.logical_not(mine))
        def _():
            send(ts.at[k], tr.at[pair], t_s, t_r, {"z": pz, "c": pc})

        @pl.when(mine)
        def _():
            tr[pair] = ts[k]

    far = sorted(range(1, nz), key=lambda k: -min(k, nz - k))

    ksum = xown[hz]
    for d in range(nx):
        for h in range(2):
            if d or h:
                wait_bytes(xr.at[d, h], x_r.at[d, h])
                ksum = ksum + xr[d, h].astype(F32)
    for k in range(nz // 2):
        for cc in range(2):
            zk[2 * k + cc] = ksum[k, rs * cc:rs * cc + rs, :].reshape(rs // 4, 4, HEAD).astype(BF16)
    slot = 2 * lax.div(z, 2) + c
    for dz in sorted(range(0, nz, 2), key=lambda k: -min(k, nz - k)):
        pz = lax.rem(z + dz, nz)
        for cc in (c, o):
            if dz or cc is o:
                send(zk.at[2 * lax.div(pz, 2) + cc], zr.at[slot], zk_s, zk_r, {"z": pz, "c": cc})
    zr[slot] = zk[slot]

    for e in range(1, ny):
        wait_bytes(yr.at[e], y_r.at[e])
    av = aw[pl.ds(HEAD, HEAD), pl.ds(0, rows)]
    for e in range(1, ny):
        av = av + yr[e].astype(F32)
    go = dot((av * tots[0]).astype(BF16), cotb[...], NN)
    wc = width // ns
    for k in range(ns):
        gos[k] = go[:, k * wc:(k + 1) * wc].astype(BF16)
    for dy in (2, 1, 3, 0):
        for dx in (2, 1, 3, 0):
            if dy < ny and dx < nx and (dy or dx):
                py, px = lax.rem(y + dy, ny), lax.rem(x + dx, nx)
                send(gos.at[py * nx + px], gor.at[s_me], go_s, go_r, {"y": py, "x": px})
    gor[s_me] = gos[s_me]

    l_swin.wait()
    row_at = lax.broadcasted_iota(jnp.int32, (rs, win), 0) + (rs * t_me - w0)
    pick = (lax.broadcasted_iota(jnp.int32, (rs, win), 1) == row_at).astype(F32).astype(BF16)
    sw = dot(pick, swin[...], NN)
    l_twin.wait()
    own_piece = mem == lax.div(z, per)

    @pl.when(own_piece)
    def _():
        wait_bytes(tr.at[pl.ds(0, nz // 2 - 1)], t_r)
        wait_bytes(ts.at[pl.ds(0, pieces - 1)], t_s)

    @pl.when(jnp.logical_not(own_piece))
    def _():
        wait_bytes(tr, t_r)
        wait_bytes(ts, t_s)

    up = jnp.sum(tr[...].astype(F32), axis=0)
    tw = twin[...].astype(F32)
    tw = jnp.where(c == 0, tw[0:rt, :], tw[rt:2 * rt, :])
    gt_o[...] = norm_back(tw, tgb[...], up)

    wait_bytes(gor.at[pl.ds(0, ns - 1)], go_r)
    go_o[...] = jnp.sum(gor[...].astype(F32), axis=0).astype(BF16)

    wait_bytes(zr.at[pl.ds(0, nz - 1)], zk_r)
    both = [zr[0].astype(F32), zr[1].astype(F32)]
    for k in range(2, nz):
        both[k % 2] = both[k % 2] + zr[k].astype(F32)
    both = jnp.concatenate([one.reshape(rs, HEAD) for one in both], axis=1).astype(BF16)
    gs_o[...] = norm_back(sw, sgb[...], dot(both, wkv[...], NT))

    for d in sends:
        d.wait_send()
    wait_bytes(gos.at[pl.ds(0, ns - 1)], go_s)
    wait_bytes(gqo.at[pl.ds(0, 4 * ny - 1)], gq_s)
    wait_bytes(zk.at[pl.ds(0, nz - 1)], zk_s)


def write_out(a, b, c, a_o, b_o, c_o, sems):
    copies = [pltpu.make_async_copy(i, j, sems.at[k]) for k, (i, j) in enumerate(((a, a_o), (b, b_o), (c, c_o)))]
    for one in copies:
        one.start()
    for one in copies:
        one.wait()


def on_device(shape, target, source, cotangent, target_gain, source_gain, w_query, w_key, w_value, w_out):
    ny, nx, nz = shape
    rows, width = target.shape
    srows = source.shape[0]
    half = srows // 2
    rt, rs = rows // (2 * nz), srows // (2 * nz)
    win = rs if rs % 8 == 0 else rs + 4
    ns = ny * nx
    wide = ny * rows
    vm = pltpu.VMEM
    sem = pltpu.SemaphoreType.DMA
    scratch = [
        vm((half, width), BF16), vm((win, width), BF16), vm((half, width), BF16),
        vm((rows, width), BF16), vm((2 * rt, width), BF16), vm((rows, width), BF16),
        vm((rows, width), BF16), vm((1, width), F32), vm((1, width), F32),
        vm((width, 2 * HEAD), BF16), vm((HEAD, width), BF16),
        vm((nx, 2, half, 2 * HEAD), BF16), vm((ny, rows, 2 * HEAD), BF16),
        vm((nx, 2, half, wide), F32), vm((nx, 2, half, wide), F32),
        vm((2, nx, 2, half, wide), BF16), vm((nx, 2, half, wide), BF16), vm((2, wide, HEAD), BF16),
        vm((ny, ny, 2, rows), F32), vm((2 * HEAD, wide), F32), vm((HEAD, wide), F32),
        vm((ny, HEAD, rows), BF16), vm((ny, HEAD, rows), BF16),
        vm((nx, srows, HEAD), F32), vm((nx, srows, HEAD), BF16), vm((nx, srows, HEAD), BF16),
        vm((nx, 2, nz // 2, 2 * rs, HEAD), BF16), vm((nx, 2, nz // 2, 2 * rs, HEAD), BF16),
        vm((2, nz // 2, 2 * rs, HEAD), F32), vm((nz, rs // 4, 4, HEAD), BF16), vm((nz, rs // 4, 4, HEAD), BF16),
        vm((4, width, HEAD), BF16), vm((4 * ny, rows // 4, HEAD), BF16), vm((4 * ny, rows // 4, HEAD), BF16),
        vm((rows // 4, width), F32), vm((rows // 4 // rt, rt, width), BF16), vm((nz // 2, rt, width), BF16),
        vm((ns, HEAD, width // ns), BF16), vm((ns, HEAD, width // ns), BF16),
        sem((11,)), sem((nx,)), sem((nx,)), sem((ny,)), sem((ny,)), sem((ny,)), sem((nx,)), sem((nx, 2)),
        sem, sem((3,)), sem, sem, sem,
        sem((nx,)), sem((nx,)), sem((ny,)), sem((ny,)), sem((ny,)), sem((nx,)), sem((nx, 2)),
        sem, sem((3,)), sem, sem, sem,
        pltpu.SemaphoreType.REGULAR, pltpu.SemaphoreType.REGULAR, pltpu.SemaphoreType.REGULAR,
        pltpu.SemaphoreType.REGULAR, pltpu.SemaphoreType.REGULAR,
    ]
    any_spec = pl.BlockSpec(memory_space=pltpu.HBM)
    vm_spec = pl.BlockSpec(memory_space=pltpu.VMEM)
    made = pl.pallas_call(
        functools.partial(kernel, (ny, nx, nz, 0, rt, rs, win)),
        out_shape=(
            vm((rt, width), BF16), vm((rs, width), BF16), vm((HEAD, width // ns), BF16),
        ),
        in_specs=[any_spec] * 9,
        out_specs=(vm_spec,) * 3,
        scratch_shapes=scratch,
        compiler_params=pltpu.CompilerParams(
            collective_id=0, has_side_effects=True, vmem_limit_bytes=56 * 1024 * 1024
        ),
    )(*(pltpu.with_memory_space_constraint(a, pltpu.HBM) for a in (
        target, source, cotangent, target_gain.reshape(1, width), source_gain.reshape(1, width),
        w_query, w_key, w_value, w_out,
    )))
    return pl.pallas_call(
        write_out,
        out_shape=tuple(jax.ShapeDtypeStruct(m.shape, m.dtype) for m in made),
        in_specs=[vm_spec] * 3,
        out_specs=(pl.BlockSpec(memory_space=pltpu.HBM),) * 3,
        scratch_shapes=[sem((3,))],
        compiler_params=pltpu.CompilerParams(vmem_limit_bytes=1024 * 1024),
    )(*made)


def solution(mesh, ny=4, nx=4):
    nz = mesh.shape["tp"] // 2
    split = Mesh(mesh.devices.reshape(ny, nx, nz, 2), ("y", "x", "z", "c"))
    sp, tp, every = ("y", "x"), ("z", "c"), ("y", "x", "z", "c")
    in_specs = (P(sp, None), P(sp, None), P(sp, None), P(), P(), P(None, tp), P(), P(), P(tp, None))
    out_specs = (P(every, None), P(every, None), P(tp, sp))
    return jax.shard_map(
        functools.partial(on_device, (ny, nx, nz)),
        mesh=split, in_specs=in_specs, out_specs=out_specs, check_vma=False,
    )
```

```python
import functools
import math

import jax
import jax.numpy as jnp
from jax import lax
from jax.experimental import pallas as pl
from jax.experimental.pallas import tpu as pltpu
from jax.sharding import Mesh
from jax.sharding import PartitionSpec as P

HEAD = 128
NORM_EPS = 1e-06
INV_ROOT = HEAD ** (-0.5)
LOG2E = math.log2(math.e)
F32, BF16 = jnp.float32, jnp.bfloat16
NN = (((1,), (0,)), ((), ()))
NT = (((1,), (1,)), ((), ()))
TN = (((0,), (0,)), ((), ()))
SHAPE = {"y": 4, "x": 4, "c": 2}


def dot(a, b, dims):
    return lax.dot_general(a, b, dims, preferred_element_type=F32)


def norm_rows(src, dst, gain):
    rows, step = src.shape[0], 16

    def one(k, carry):
        at = pl.ds(pl.multiple_of(k * step, step), step)
        v = src[at, :].astype(F32)
        r = lax.rsqrt(jnp.mean(v * v, axis=1, keepdims=True) + NORM_EPS)
        dst[at, :] = (v * r * gain[...]).astype(BF16)
        return carry

    lax.fori_loop(0, rows // step, one, 0, unroll=4)


def norm_back(rows, gain, upstream):
    r = lax.rsqrt(jnp.mean(rows * rows, axis=1, keepdims=True) + NORM_EPS)
    unit = rows * r
    pulled = upstream * gain
    return (r * (pulled - unit * jnp.mean(pulled * unit, axis=1, keepdims=True))).astype(BF16)


def wait_bytes(ref, sem):
    pltpu.make_async_copy(ref, ref, sem).wait()


def kernel(
    dims, tgt_h, src_h, cot_h, tg_h, sg_h, wq_h, wk_h, wv_h, wo_h,
    gt_o, gs_o, go_o,
    srcb, swin, sn, tgtb, twin, tn, cotb, tgb, sgb, wkv, wob,
    kv, qg, est, pgt, lhs, t_b, rhs, stat, aw, tk,
    ys, yr, gkv, ps, pr, xs, xr, xown, zk, zr,
    wq4, gqo, gqi, pmat, ts, tr, gos, gor,
    ld, kv_r, kvp_r, qg_r, st_r, y_r, ps_r, x_r, zk_r, wq_r, gq_r, t_r, go_r,
    kv_s, kvp_s, qg_s, st_s, y_s, ps_s, x_s, zk_s, wq_s, gq_s, t_s, go_s,
    up_1, up_2, up_4, seen_x, seen_y,
):
    ny, nx, nz, gsz, rt, rs, win = dims
    ns = ny * nx
    y, x, z, c = (lax.axis_index(a) for a in ("y", "x", "z", "c"))
    o = 1 - c
    s_me = y * nx + x
    zo = z + 1 - 2 * lax.rem(z, 2)
    zf = lax.rem(z - 1 + 2 * lax.rem(z, 2) + nz, nz)
    hz = lax.rem(z, 2)
    mem = 2 * hz + c
    zp = lax.select(c == 0, zo, zf)
    half = kv.shape[2]
    rows = tgtb.shape[0]
    width = tgtb.shape[1]

    barrier = pltpu.get_barrier_semaphore()

    def signal(sem, to):
        pl.semaphore_signal(sem, inc=1, device_id=to, device_id_type=pl.DeviceIdType.MESH)

    def beside(k):
        return [lax.rem(z + k, nz), lax.rem(z + nz - k, nz)] if 2 * k < nz else [lax.rem(z + k, nz)]

    peers = [{"c": o}]
    x_peers = [{"x": lax.rem(x + dx, nx)} for dx in range(1, nx)]
    y_peers = [{"y": lax.rem(y + dy, ny)} for dy in range(1, ny)]
    peers.extend(x_peers + y_peers)
    for pz in [zo, zf] if nz > 2 else [zo]:
        peers.extend([{"z": pz, "c": c}, {"z": pz, "c": o}])
    for peer in peers:
        signal(barrier, peer)

    def load(k, a, b):
        d = pltpu.make_async_copy(a, b, ld.at[k])
        d.start()
        return d

    t_me = 2 * z + c
    w0 = pl.multiple_of(lax.div(rs * t_me, 8) * 8, 8)
    l_tgt = load(4, tgt_h, tgtb)
    l_tg = load(5, tg_h, tgb)
    l_wq = load(6, wq_h, wq4.at[mem])
    l_cot = load(7, cot_h, cotb)
    l_wo = load(8, wo_h, wob)
    l_src = load(0, src_h.at[pl.ds(pl.multiple_of(c * half, half), half), :], srcb)
    l_sg = load(1, sg_h, sgb)
    l_wk = load(2, wk_h, wkv.at[:, pl.ds(0, HEAD)])
    l_wv = load(3, wv_h, wkv.at[:, pl.ds(HEAD, HEAD)])
    l_swin = load(9, src_h.at[pl.ds(w0, win), :], swin)
    l_twin = load(10, tgt_h.at[pl.ds(pl.multiple_of(2 * rt * z, 2 * rt), 2 * rt), :], twin)

    def send(a, b, s_sem, r_sem, to):
        d = pltpu.make_async_remote_copy(
            src_ref=a, dst_ref=b, send_sem=s_sem, recv_sem=r_sem,
            device_id=to, device_id_type=pl.DeviceIdType.MESH,
        )
        d.start()
        return d

    l_tgt.wait()
    l_tg.wait()
    norm_rows(tgtb, tn, tgb)
    l_wq.wait()
    qg[0, :, pl.ds(0, HEAD)] = dot(tn[...], wq4[mem], NN).astype(BF16)
    l_cot.wait()
    l_wo.wait()
    qg[0, :, pl.ds(HEAD, HEAD)] = dot(cotb[...], wob[...], NT).astype(BF16)
    pl.semaphore_wait(barrier, len(peers))
    sends = []
    x_order = [d for d in (1, 3, 2) if d < nx]
    y_order = [d for d in (2, 1, 3) if d < ny]
    for d in y_order:
        sends.append(send(qg.at[0], qg.at[d], qg_s.at[d], qg_r.at[d], {"y": lax.rem(y + d, ny)}))
    for peer in y_peers:
        signal(seen_y, peer)
    for peer in x_peers:
        signal(seen_x, peer)
    for pz in beside(1):
        signal(up_1, {"z": pz})
    sends.append(send(wq4.at[mem], wq4.at[mem], wq_s.at[0], wq_r.at[0], {"z": zo}))
    sends.append(send(wq4.at[mem], wq4.at[mem], wq_s.at[1], wq_r.at[1], {"c": o}))
    l_src.wait()
    l_sg.wait()
    norm_rows(srcb, sn, sgb)
    l_wk.wait()
    l_wv.wait()
    kv[0, c] = dot(sn[...], wkv[...], NN).astype(BF16)
    for d in x_order:
        sends.append(send(kv.at[0, c], kv.at[d, c], kv_s.at[d], kv_r.at[d], {"x": lax.rem(x + d, nx)}))
    sends.append(send(kv.at[0, c], kv.at[0, c], kvp_s.at[0], kvp_r.at[0], {"c": o}))
    pl.semaphore_wait(up_1, len(beside(1)))
    for pz in beside(2):
        signal(up_2, {"z": pz})

    for d in range(1, ny):
        wait_bytes(qg.at[d], qg_r.at[d])
    pl.semaphore_wait(up_2, len(beside(2)))
    for pz in beside(4):
        signal(up_4, {"z": pz})
    q_all = qg[:, :, pl.ds(0, HEAD)].reshape(ny * rows, HEAD)
    g_all = qg[:, :, pl.ds(HEAD, HEAD)].reshape(ny * rows, HEAD)
    tot = jnp.zeros((1, ny * rows), F32)
    tilt = jnp.zeros((1, ny * rows), F32)

    def unit(d, h, tot, tilt):
        key, val = kv[d, h, :, pl.ds(0, HEAD)], kv[d, h, :, pl.ds(HEAD, HEAD)]
        e = jnp.exp2(dot(key, q_all, NT) * (INV_ROOT * LOG2E) - 2.0)
        g = dot(val, g_all, NT)
        t = e * g
        est[d, h] = e
        pgt[d, h] = g
        lhs[1, d, h] = e.astype(BF16)
        t_b[d, h] = t.astype(BF16)
        return tot + jnp.sum(e, axis=0, keepdims=True), tilt + jnp.sum(t, axis=0, keepdims=True)

    def unit_sums(d, h, first):
        both = dot(kv[d, h], lhs[1, d, h], TN)
        one = dot(kv[d, h, :, pl.ds(0, HEAD)], t_b[d, h], TN)
        aw[...] = both if first else aw[...] + both
        tk[...] = one if first else tk[...] + one

    x_seen = [d for d in (1, 3, 2) if d < nx]
    tot, tilt = unit(0, c, tot, tilt)
    before = 0
    for d in x_seen:
        wait_bytes(kv.at[d, c], kv_r.at[d])
        sends.append(send(kv.at[d, c], kv.at[d, c], kvp_s.at[d], kvp_r.at[d], {"c": o}))
        wait_bytes(kv.at[before, o], kvp_r.at[before])
        tot, tilt = unit(before, o, tot, tilt)
        tot, tilt = unit(d, c, tot, tilt)
        before = d
    wait_bytes(kv.at[before, o], kvp_r.at[before])
    tot, tilt = unit(before, o, tot, tilt)

    for e in range(ny):
        stat[0, e, 0:1, :] = tot[:, e * rows:(e + 1) * rows]
        stat[0, e, 1:2, :] = tilt[:, e * rows:(e + 1) * rows]
    for d in y_order:
        sends.append(send(stat.at[0], stat.at[d], st_s.at[d], st_r.at[d], {"y": lax.rem(y + d, ny)}))
    for d in range(nx):
        for h in range(2):
            unit_sums(d, h, d + h == 0)
    for e in y_order:
        ys[e] = aw[pl.ds(HEAD, HEAD), pl.ds(e * rows, rows)].astype(BF16)
        sends.append(send(ys.at[e], yr.at[e], y_s.at[e], y_r.at[e], {"y": lax.rem(y + ny - e, ny)}))
    for d in range(1, ny):
        wait_bytes(stat.at[d], st_r.at[d])
    tots, deltas = [], []
    for e in range(ny):
        both = stat[0, e]
        for d in range(1, ny):
            both = both + stat[d, (e - d) % ny]
        tots.append(1.0 / both[0:1, :])
        deltas.append(both[1:2, :] / both[0:1, :])
    inv_total = jnp.concatenate(tots, axis=1)
    delta = jnp.concatenate(deltas, axis=1)

    pl.semaphore_wait(seen_y, len(y_peers))
    gq = ((tk[...] - delta * aw[pl.ds(0, HEAD), :]) * (inv_total * INV_ROOT)).T.astype(BF16)
    quarter = rows // 4
    for e in range(ny):
        for k in range(4):
            gqo[4 * e + k] = gq[e * rows + k * quarter:e * rows + (k + 1) * quarter, :]
    for e in y_order + [0]:
        py = lax.rem(y + ny - e, ny)
        for step in (2, 3, 1, 0):
            if e or step:
                pz = zo if step > 1 else z
                pc = o if step % 2 else c
                to = 2 * lax.rem(pz, 2) + pc
                send(gqo.at[4 * e + to], gqi.at[4 * e + mem], gq_s, gq_r, {"y": py, "z": pz, "c": pc})
    gqi[mem] = gqo[mem]
    pl.semaphore_wait(seen_x, len(x_peers))
    rhs[0] = q_all
    rhs[1] = g_all
    root = lax.select(c == 0, jnp.float32(INV_ROOT), jnp.float32(1.0))
    root_o = lax.select(c == 0, jnp.float32(1.0), jnp.float32(INV_ROOT))
    order = [d for d in (2, 1, 3, 0) if d < nx]

    def other(d):
        for h in range(2):
            p = est[d, h] * inv_total
            lhs[0, d, h] = (p * (pgt[d, h] - delta)).astype(BF16)
            lhs[1, d, h] = p.astype(BF16)
            ps[d, pl.ds(h * half, half), :] = (dot(lhs[o, d, h], rhs[o], NN) * root_o).astype(BF16)
        sends.append(send(ps.at[d], pr.at[d], ps_s.at[d], ps_r.at[d], {"c": o}))

    def own(d):
        for h in range(2):
            gkv[d, pl.ds(h * half, half), :] = dot(lhs[c, d, h], rhs[c], NN) * root

    def pass_on(d):
        wait_bytes(pr.at[d], ps_r.at[d])
        mine = gkv[d] + pr[d].astype(F32)
        mine = mine.reshape(nz // 2, 2, 2 * rs, HEAD)
        px = lax.rem(x + nx - d, nx)
        for h in range(2):
            if d == 0:
                xown[h] = mine[:, h]
            xs[d, h] = mine[:, h].astype(BF16)
        sends.append(send(xs.at[d, 1 - hz], xr.at[d, 1], x_s.at[d, 1], x_r.at[d, 1], {"x": px, "z": zp}))
        if d:
            sends.append(send(xs.at[d, hz], xr.at[d, 0], x_s.at[d, 0], x_r.at[d, 0], {"x": px}))

    steps = [(other, order[0])]
    for i in range(len(order)):
        if i + 1 < len(order):
            steps.append((other, order[i + 1]))
        if i:
            steps.append((pass_on, order[i - 1]))
        steps.append((own, order[i]))
    for step, d in steps[:5]:
        step(d)
    wait_bytes(wq4.at[0], wq_r.at[0])
    mem_z = 2 * lax.rem(zo, 2) + c
    sends.append(send(wq4.at[mem_z], wq4.at[mem_z], wq_s.at[2], wq_r.at[2], {"c": o}))
    for step, d in steps[5:]:
        step(d)
    pass_on(order[-1])
    wait_bytes(gqi.at[pl.ds(0, 4 * ny - 1)], gq_r)
    wait_bytes(wq4.at[0], wq_r.at[1])
    wait_bytes(wq4.at[0], wq_r.at[2])
    up = None
    for k in range(4):
        one = gqi[k].astype(F32)
        for e in range(1, ny):
            one = one + gqi[4 * e + k].astype(F32)
        one = dot(one.astype(BF16), wq4[k], NT)
        up = one if up is None else up + one
    pmat[...] = up
    pieces = quarter // rt
    for k in range(pieces):
        ts[k] = pmat[pl.ds(rt * k, rt), :].astype(BF16)
    pl.semaphore_wait(up_4, len(beside(4)))
    pair = lax.div(z, 2)
    per = pieces // 2
    for k in range(pieces):
        pz, pc = per * mem + k // 2, k % 2
        mine = jnp.logical_and(pz == z, pc == c)

        @pl.when(jnp.logical_not(mine))
        def _():
            send(ts.at[k], tr.at[pair], t_s, t_r, {"z": pz, "c": pc})

        @pl.when(mine)
        def _():
            tr[pair] = ts[k]

    far = sorted(range(1, nz), key=lambda k: -min(k, nz - k))

    ksum = xown[hz]
    for d in range(nx):
        for h in range(2):
            if d or h:
                wait_bytes(xr.at[d, h], x_r.at[d, h])
                ksum = ksum + xr[d, h].astype(F32)
    for k in range(nz // 2):
        for cc in range(2):
            zk[2 * k + cc] = ksum[k, rs * cc:rs * cc + rs, :].reshape(rs // 4, 4, HEAD).astype(BF16)
    slot = 2 * lax.div(z, 2) + c
    for dz in sorted(range(0, nz, 2), key=lambda k: -min(k, nz - k)):
        pz = lax.rem(z + dz, nz)
        for cc in (c, o):
            if dz or cc is o:
                send(zk.at[2 * lax.div(pz, 2) + cc], zr.at[slot], zk_s, zk_r, {"z": pz, "c": cc})
    zr[slot] = zk[slot]

    for e in range(1, ny):
        wait_bytes(yr.at[e], y_r.at[e])
    av = aw[pl.ds(HEAD, HEAD), pl.ds(0, rows)]
    for e in range(1, ny):
        av = av + yr[e].astype(F32)
    go = dot((av * tots[0]).astype(BF16), cotb[...], NN)
    wc = width // ns
    for k in range(ns):
        gos[k] = go[:, k * wc:(k + 1) * wc].astype(BF16)
    for dy in (2, 1, 3, 0):
        for dx in (2, 1, 3, 0):
            if dy < ny and dx < nx and (dy or dx):
                py, px = lax.rem(y + dy, ny), lax.rem(x + dx, nx)
                send(gos.at[py * nx + px], gor.at[s_me], go_s, go_r, {"y": py, "x": px})
    gor[s_me] = gos[s_me]

    l_swin.wait()
    row_at = lax.broadcasted_iota(jnp.int32, (rs, win), 0) + (rs * t_me - w0)
    pick = (lax.broadcasted_iota(jnp.int32, (rs, win), 1) == row_at).astype(F32).astype(BF16)
    sw = dot(pick, swin[...], NN)
    l_twin.wait()
    own_piece = mem == lax.div(z, per)

    @pl.when(own_piece)
    def _():
        wait_bytes(tr.at[pl.ds(0, nz // 2 - 1)], t_r)
        wait_bytes(ts.at[pl.ds(0, pieces - 1)], t_s)

    @pl.when(jnp.logical_not(own_piece))
    def _():
        wait_bytes(tr, t_r)
        wait_bytes(ts, t_s)

    up = jnp.sum(tr[...].astype(F32), axis=0)
    tw = twin[...].astype(F32)
    tw = jnp.where(c == 0, tw[0:rt, :], tw[rt:2 * rt, :])
    gt_o[...] = norm_back(tw, tgb[...], up)

    wait_bytes(gor.at[pl.ds(0, ns - 1)], go_r)
    go_o[...] = jnp.sum(gor[...].astype(F32), axis=0).astype(BF16)

    wait_bytes(zr.at[pl.ds(0, nz - 1)], zk_r)
    both = [zr[0].astype(F32), zr[1].astype(F32)]
    for k in range(2, nz):
        both[k % 2] = both[k % 2] + zr[k].astype(F32)
    both = jnp.concatenate([one.reshape(rs, HEAD) for one in both], axis=1).astype(BF16)
    gs_o[...] = norm_back(sw, sgb[...], dot(both, wkv[...], NT))

    for d in sends:
        d.wait_send()
    wait_bytes(gos.at[pl.ds(0, ns - 1)], go_s)
    wait_bytes(gqo.at[pl.ds(0, 4 * ny - 1)], gq_s)
    wait_bytes(zk.at[pl.ds(0, nz - 1)], zk_s)


def write_out(a, b, c, a_o, b_o, c_o, sems):
    copies = [pltpu.make_async_copy(i, j, sems.at[k]) for k, (i, j) in enumerate(((a, a_o), (b, b_o), (c, c_o)))]
    for one in copies:
        one.start()
    for one in copies:
        one.wait()


def on_device(shape, target, source, cotangent, target_gain, source_gain, w_query, w_key, w_value, w_out):
    ny, nx, nz = shape
    rows, width = target.shape
    srows = source.shape[0]
    half = srows // 2
    rt, rs = rows // (2 * nz), srows // (2 * nz)
    win = rs if rs % 8 == 0 else rs + 4
    ns = ny * nx
    wide = ny * rows
    vm = pltpu.VMEM
    sem = pltpu.SemaphoreType.DMA
    scratch = [
        vm((half, width), BF16), vm((win, width), BF16), vm((half, width), BF16),
        vm((rows, width), BF16), vm((2 * rt, width), BF16), vm((rows, width), BF16),
        vm((rows, width), BF16), vm((1, width), F32), vm((1, width), F32),
        vm((width, 2 * HEAD), BF16), vm((HEAD, width), BF16),
        vm((nx, 2, half, 2 * HEAD), BF16), vm((ny, rows, 2 * HEAD), BF16),
        vm((nx, 2, half, wide), F32), vm((nx, 2, half, wide), F32),
        vm((2, nx, 2, half, wide), BF16), vm((nx, 2, half, wide), BF16), vm((2, wide, HEAD), BF16),
        vm((ny, ny, 2, rows), F32), vm((2 * HEAD, wide), F32), vm((HEAD, wide), F32),
        vm((ny, HEAD, rows), BF16), vm((ny, HEAD, rows), BF16),
        vm((nx, srows, HEAD), F32), vm((nx, srows, HEAD), BF16), vm((nx, srows, HEAD), BF16),
        vm((nx, 2, nz // 2, 2 * rs, HEAD), BF16), vm((nx, 2, nz // 2, 2 * rs, HEAD), BF16),
        vm((2, nz // 2, 2 * rs, HEAD), F32), vm((nz, rs // 4, 4, HEAD), BF16), vm((nz, rs // 4, 4, HEAD), BF16),
        vm((4, width, HEAD), BF16), vm((4 * ny, rows // 4, HEAD), BF16), vm((4 * ny, rows // 4, HEAD), BF16),
        vm((rows // 4, width), F32), vm((rows // 4 // rt, rt, width), BF16), vm((nz // 2, rt, width), BF16),
        vm((ns, HEAD, width // ns), BF16), vm((ns, HEAD, width // ns), BF16),
        sem((11,)), sem((nx,)), sem((nx,)), sem((ny,)), sem((ny,)), sem((ny,)), sem((nx,)), sem((nx, 2)),
        sem, sem((3,)), sem, sem, sem,
        sem((nx,)), sem((nx,)), sem((ny,)), sem((ny,)), sem((ny,)), sem((nx,)), sem((nx, 2)),
        sem, sem((3,)), sem, sem, sem,
        pltpu.SemaphoreType.REGULAR, pltpu.SemaphoreType.REGULAR, pltpu.SemaphoreType.REGULAR,
        pltpu.SemaphoreType.REGULAR, pltpu.SemaphoreType.REGULAR,
    ]
    any_spec = pl.BlockSpec(memory_space=pltpu.HBM)
    vm_spec = pl.BlockSpec(memory_space=pltpu.VMEM)
    made = pl.pallas_call(
        functools.partial(kernel, (ny, nx, nz, 0, rt, rs, win)),
        out_shape=(
            vm((rt, width), BF16), vm((rs, width), BF16), vm((HEAD, width // ns), BF16),
        ),
        in_specs=[any_spec] * 9,
        out_specs=(vm_spec,) * 3,
        scratch_shapes=scratch,
        compiler_params=pltpu.CompilerParams(
            collective_id=0, has_side_effects=True, vmem_limit_bytes=56 * 1024 * 1024
        ),
    )(*(pltpu.with_memory_space_constraint(a, pltpu.HBM) for a in (
        target, source, cotangent, target_gain.reshape(1, width), source_gain.reshape(1, width),
        w_query, w_key, w_value, w_out,
    )))
    return pl.pallas_call(
        write_out,
        out_shape=tuple(jax.ShapeDtypeStruct(m.shape, m.dtype) for m in made),
        in_specs=[vm_spec] * 3,
        out_specs=(pl.BlockSpec(memory_space=pltpu.HBM),) * 3,
        scratch_shapes=[sem((3,))],
        compiler_params=pltpu.CompilerParams(vmem_limit_bytes=1024 * 1024),
    )(*made)


def solution(mesh, ny=4, nx=4):
    nz = mesh.shape["tp"] // 2
    split = Mesh(mesh.devices.reshape(ny, nx, nz, 2), ("y", "x", "z", "c"))
    sp, tp, every = ("y", "x"), ("z", "c"), ("y", "x", "z", "c")
    in_specs = (P(sp, None), P(sp, None), P(sp, None), P(), P(), P(None, tp), P(), P(), P(tp, None))
    out_specs = (P(every, None), P(every, None), P(tp, sp))
    return jax.shard_map(
        functools.partial(on_device, (ny, nx, nz)),
        mesh=split, in_specs=in_specs, out_specs=out_specs, check_vma=False,
    )
```
